512 devices in a mesh: sp: 16 (over z), fs: 4 (over y), tp: 8 (over x, core).
Axes of the slice: x: 4, y: 4, z: 16, core: 2. Of those that a mesh axis runs over, the one named last changes fastest.
Arguments:
- stream: bfloat16 [4, 4096, 2048], P('fs', 'sp'), may hold values from -6 to 6
- norm_gain: bfloat16 [2048], replicated, may hold values from 0.099609375 to 1.8984375
- query_weight: bfloat16 [2048, 1024], P(None, 'tp'), may hold values from -0.125 to 0.125
- key_weight: bfloat16 [2048, 1024], P(None, 'tp'), may hold values from -0.125 to 0.125
- value_weight: bfloat16 [2048, 1024], P(None, 'tp'), may hold values from -0.125 to 0.125
- filter_input: bfloat16 [2048, 1024], P(None, 'tp'), may hold values from -0.125 to 0.125
- filter_gate: bfloat16 [2048, 1024], P(None, 'tp'), may hold values from -0.125 to 0.125
- score_offset: bfloat16 [4, 4096, 16], P('fs', 'sp', 'tp'), may hold values from -16 to 0
- head_gain: bfloat16 [1024], P('tp'), may hold values from 0.099609375 to 1.8984375
- filter_taps: bfloat16 [31, 1024], P(None, 'tp'), may hold values from -5 to 5
- channel_gain: bfloat16 [1024], P('tp'), may hold values from 0.099609375 to 1.8984375
- channel_shift: bfloat16 [1024], P('tp'), may hold values from -3 to 3
- attend_out: bfloat16 [1024, 2048], P('tp'), may hold values from -0.125 to 0.125
- filter_out: bfloat16 [1024, 2048], P('tp'), may hold values from -0.125 to 0.125
Outputs:
- mixed_out: bfloat16 [4, 4096, 2048], P('fs', ('sp', 'tp'))
- mass_log: float32 [4, 4096, 16], P('fs', 'sp', 'tp')
The draws below stay inside these ranges and needn't reach their ends.
All inputs are finite; a program needn't handle non-finite values.
Results may differ from the reference program's by a relative error of at most 0.015.
Values may be sent and summed in bfloat16 or wider, within the bound.
A program may use at most 64 MiB of HBM per device.

```python
import math
import jax
import jax.numpy as jnp
from jax import lax

D = 2048
HEAD_COUNT = 16
HEAD_DIM = 64
CONV = 1024
KERNEL = 31
TOK_DEV = 256
ATTN = 1024
SEQUENCE_LENGTH = 4096
SEQUENCE_COUNT = 4


def draw_score_offset(key, part):
    key_collection = jax.random.split(jax.random.fold_in(key, 3), 4)
    slow_share = 0.5
    slowly = jax.random.bernoulli(key_collection[0], slow_share, (SEQUENCE_COUNT, 1, HEAD_COUNT))
    levels = jnp.where(slowly, math.log(0.15 / SEQUENCE_LENGTH), math.log(1.0 / 40.0))
    blocks = SEQUENCE_LENGTH // TOK_DEV
    shifts = jax.random.uniform(key_collection[1], (SEQUENCE_COUNT, blocks, 1, HEAD_COUNT), jnp.float32, -0.7, 0.7)
    shifts = jnp.broadcast_to(shifts, (SEQUENCE_COUNT, blocks, TOK_DEV, HEAD_COUNT)).reshape(SEQUENCE_COUNT, SEQUENCE_LENGTH, HEAD_COUNT)
    jitter = jax.random.uniform(key_collection[2], (SEQUENCE_COUNT, SEQUENCE_LENGTH, HEAD_COUNT), jnp.float32, -1.0, 1.0)
    break_fractions = jax.random.randint(key_collection[3], (SEQUENCE_COUNT, 4, 1, HEAD_COUNT), 0, SEQUENCE_LENGTH)
    slot_positions = jnp.arange(SEQUENCE_LENGTH, dtype=jnp.int32)[None, None, :, None]
    broken_weights = jnp.any(slot_positions == break_fractions, axis=1)
    values = jnp.where(broken_weights, -0.6 + 0.3 * jitter, levels + shifts + jitter)
    return values.astype(jnp.bfloat16)


def draw_filter_taps(key, part):
    entry_key, scale_key = jax.random.split(jax.random.fold_in(key, 7))
    channel = jnp.arange(CONV, dtype=jnp.float32) / CONV
    roughness = jax.random.uniform(scale_key, (1, CONV), jnp.float32, 0.7, 1.4)
    entries = jnp.clip(jax.random.normal(entry_key, (KERNEL, CONV), jnp.float32), -4.0, 4.0)
    scaling = 4.0 ** channel
    return (entries * scaling[None, :] * roughness / math.sqrt(KERNEL)).astype(jnp.bfloat16)


def block_scale(rng, shape, cuts, smallest, top_value):
    factor_of = 1.0
    for dim, shards_of in cuts:
        draws = jax.random.uniform(jax.random.fold_in(jax.random.fold_in(rng, 6), dim), (shards_of,), jnp.float32, smallest / len(cuts), top_value / len(cuts))
        factor_of = factor_of * jnp.repeat(jnp.exp(draws), shape[dim] // shards_of).reshape((-1,) + (1,) * (len(shape) - 1 - dim))
    return factor_of


def normal_values(own_key, dims, width, reach, shards=(), kind=jnp.bfloat16):
    array = width * jax.random.normal(own_key, dims, jnp.float32)
    if shards:
        array = array * block_scale(own_key, dims, shards, -0.22, 0.18)
    return jnp.clip(array, -reach, reach).astype(kind)


def setup_inputs(seed: int = 0) -> dict:
    key_of = jax.random.split(jax.random.key(seed), 15)
    return {
        "stream": normal_values(key_of[0], (SEQUENCE_COUNT, SEQUENCE_LENGTH, D), 1.0, 6.0, ((0, 4), (1, 16))),
        "norm_gain": jnp.clip(1.0 + 0.18 * jax.random.normal(key_of[1], (D,), jnp.float32), 0.099609375, 1.8984375).astype(jnp.bfloat16),
        "query_weight": normal_values(key_of[2], (D, ATTN), D ** -0.5, 0.125, ((1, 8),)),
        "key_weight": normal_values(key_of[3], (D, ATTN), D ** -0.5, 0.125, ((1, 8),)),
        "value_weight": normal_values(key_of[4], (D, ATTN), D ** -0.5, 0.125, ((1, 8),)),
        "filter_input": normal_values(key_of[5], (D, CONV), D ** -0.5, 0.125, ((1, 8),)),
        "filter_gate": normal_values(key_of[6], (D, CONV), D ** -0.5, 0.125, ((1, 8),)),
        "score_offset": draw_score_offset(jax.random.fold_in(key_of[14], 71), 0),
        "head_gain": jnp.clip(1.0 + 0.18 * jax.random.normal(key_of[8], (ATTN,), jnp.float32), 0.099609375, 1.8984375).astype(jnp.bfloat16),
        "filter_taps": draw_filter_taps(jax.random.fold_in(key_of[14], 71), 0),
        "channel_gain": jnp.clip(1.0 + 0.18 * jax.random.normal(key_of[10], (CONV,), jnp.float32), 0.099609375, 1.8984375).astype(jnp.bfloat16),
        "channel_shift": normal_values(key_of[11], (CONV,), 0.5, 3.0, ((0, 8),)),
        "attend_out": normal_values(key_of[12], (ATTN, D), (ATTN + CONV) ** -0.5, 0.125, ((0, 8),)),
        "filter_out": normal_values(key_of[13], (CONV, D), (ATTN + CONV) ** -0.5, 0.125, ((0, 8),)),
    }


rms_eps = 1e-06
norm_eps = 1e-05
mass_floor = 0.01

def attend_sequence(queries, keys_seq, values_seq, offsets):
    query_block = min(512, SEQUENCE_LENGTH)
    qfloat = queries.astype(jnp.float32).reshape(SEQUENCE_LENGTH, HEAD_COUNT, HEAD_DIM)
    kfloat = keys_seq.astype(jnp.float32).reshape(SEQUENCE_LENGTH, HEAD_COUNT, HEAD_DIM)
    vfloat = values_seq.astype(jnp.float32).reshape(SEQUENCE_LENGTH, HEAD_COUNT, HEAD_DIM)
    offsets_t = offsets.astype(jnp.float32).T
    key_pos = jnp.arange(SEQUENCE_LENGTH, dtype=jnp.int32)

    def one_block(block_index):
        first_row = (block_index * query_block).astype(jnp.int32)
        qpart = lax.dynamic_slice_in_dim(qfloat, first_row, query_block, 0)
        scores = jnp.einsum('thd,shd->hts', qpart, kfloat, precision=lax.Precision.HIGHEST) * HEAD_DIM ** (-0.5)
        scores = scores + offsets_t[:, None, :]
        query_pos = first_row + jnp.arange(query_block, dtype=jnp.int32)
        strict = key_pos[None, :] < query_pos[:, None]
        losing = jnp.where(strict[None], jax.nn.log_sigmoid(-scores), 0.0)
        beyond = lax.cumsum(losing, axis=2, reverse=True) - losing
        weights = jnp.where(strict[None], jnp.exp(jax.nn.log_sigmoid(scores) + beyond), 0.0)
        weight_mass = lax.optimization_barrier(jnp.sum(weights, axis=2))
        rounded = lax.optimization_barrier(weights.astype(jnp.bfloat16)).astype(jnp.float32)
        attended = jnp.einsum('hts,shd->thd', rounded, vfloat, precision=lax.Precision.HIGHEST)
        return (attended, weight_mass.T)
    attended, weight_mass = lax.map(one_block, jnp.arange(SEQUENCE_LENGTH // query_block, dtype=jnp.int32))
    return (attended.reshape(SEQUENCE_LENGTH, HEAD_COUNT, HEAD_DIM), weight_mass.reshape(SEQUENCE_LENGTH, HEAD_COUNT))

def reference(stream, norm_gain, query_weight, key_weight, value_weight, filter_input, filter_gate, score_offset, head_gain, filter_taps, channel_gain, channel_shift, attend_out, filter_out):
    xfloat = stream.astype(jnp.float32)
    normed = xfloat * lax.rsqrt(lax.optimization_barrier(jnp.mean(xfloat * xfloat, axis=-1, keepdims=True)) + rms_eps)
    normed = (normed * norm_gain.astype(jnp.float32)).astype(jnp.bfloat16)
    flat = normed.reshape(SEQUENCE_COUNT * SEQUENCE_LENGTH, D)

    def project(weight):
        return jnp.dot(flat, weight, preferred_element_type=jnp.float32).astype(jnp.bfloat16)
    queries = project(query_weight).reshape(SEQUENCE_COUNT, SEQUENCE_LENGTH, ATTN)
    keys_all = project(key_weight).reshape(SEQUENCE_COUNT, SEQUENCE_LENGTH, ATTN)
    values_all = project(value_weight).reshape(SEQUENCE_COUNT, SEQUENCE_LENGTH, ATTN)
    conv_values = project(filter_input)
    conv_gates = project(filter_gate)

    def per_sequence(seq_index):
        return attend_sequence(queries[seq_index], keys_all[seq_index], values_all[seq_index], score_offset[seq_index])
    attended, weight_mass = lax.map(per_sequence, jnp.arange(SEQUENCE_COUNT, dtype=jnp.int32))
    head_scale = lax.rsqrt(lax.optimization_barrier(jnp.mean(attended * attended, axis=-1, keepdims=True)) + rms_eps)
    heads_out = attended * head_scale * head_gain.astype(jnp.float32).reshape(HEAD_COUNT, HEAD_DIM)
    heads_out = heads_out.astype(jnp.bfloat16).reshape(SEQUENCE_COUNT * SEQUENCE_LENGTH, ATTN)
    mass_log = jnp.log(jnp.maximum(weight_mass, mass_floor))
    gated_rows = (conv_values.astype(jnp.float32) * jax.nn.sigmoid(conv_gates.astype(jnp.float32))).astype(jnp.bfloat16)
    gated_rows = gated_rows.reshape(SEQUENCE_COUNT, SEQUENCE_LENGTH, CONV)
    padded = jnp.pad(gated_rows.astype(jnp.float32), ((0, 0), (KERNEL - 1, 0), (0, 0)))
    tap_values = filter_taps.astype(jnp.float32)
    filtered = jnp.zeros((SEQUENCE_COUNT, SEQUENCE_LENGTH, CONV), jnp.float32)
    for tap_index in range(KERNEL):
        filtered = filtered + padded[:, tap_index:tap_index + SEQUENCE_LENGTH] * tap_values[tap_index]
    center = lax.optimization_barrier(jnp.mean(filtered, axis=-1, keepdims=True))
    deviation = filtered - center
    spread = lax.optimization_barrier(jnp.mean(deviation * deviation, axis=-1, keepdims=True))
    conv_out = jax.nn.silu(deviation * lax.rsqrt(spread + norm_eps) * channel_gain.astype(jnp.float32) + channel_shift.astype(jnp.float32)).astype(jnp.bfloat16)
    conv_out = conv_out.reshape(SEQUENCE_COUNT * SEQUENCE_LENGTH, CONV)
    mixed_out = jnp.dot(heads_out, attend_out, preferred_element_type=jnp.float32)
    mixed_out = mixed_out + jnp.dot(conv_out, filter_out, preferred_element_type=jnp.float32)
    return (mixed_out.astype(jnp.bfloat16).reshape(SEQUENCE_COUNT, SEQUENCE_LENGTH, D), mass_log)
```

```python
import functools

import jax
import jax.numpy as jnp
from jax import lax
from jax.experimental import pallas as pl
from jax.experimental.pallas import tpu as pltpu
from jax.sharding import PartitionSpec as P

HEAD_DIM = 64

rms_eps = 1e-06
norm_eps = 1e-05
mass_floor = 0.01

MESH = pl.DeviceIdType.MESH
f32 = jnp.float32
bf16 = jnp.bfloat16


def dot_nt(a, b):
    return lax.dot_general(a, b, (((1,), (1,)), ((), ())), preferred_element_type=f32)


def kernel(
    n,
    tps,
    x_hbm,
    gain_ref,
    wq_hbm,
    wk_hbm,
    wv_hbm,
    wi_hbm,
    wg_hbm,
    off_ref,
    head_gain_ref,
    taps_ref,
    cgain_ref,
    cshift_ref,
    ao_hbm,
    fo_hbm,
    out_ref,
    mass_ref,
    x_v,
    normed,
    w_v,
    wcat,
    kbuf,
    vbuf,
    obuf,
    qs,
    tri,
    acc_r,
    sum_r,
    acc_l,
    sum_l,
    gated,
    halo,
    ext,
    filt,
    stat_send,
    stat_recv,
    cat,
    part,
    recv,
    load_sem,
    plus_send,
    plus_recv,
    minus_send,
    minus_recv,
    halo_sem,
    stat_ssem,
    stat_rsem,
    rs_ssem,
    rs_rsem,
):
    rows = x_hbm.shape[0]
    width = wq_hbm.shape[1]
    reach = taps_ref.shape[0] - 1
    me = lax.axis_index("sp")
    tp = lax.axis_index("tp")
    right = lax.rem(me + 1, n)
    left = lax.rem(me + n - 1, n)
    dist = n // 2
    low = n - dist - 2

    loads = [
        (x_hbm, x_v),
        (wk_hbm, w_v.at[:, 0:width]),
        (wv_hbm, w_v.at[:, width : 2 * width]),
        (wq_hbm, w_v.at[:, 2 * width : 3 * width]),
        (wi_hbm, w_v.at[:, 3 * width : 4 * width]),
        (wg_hbm, w_v.at[:, 4 * width : 5 * width]),
        (ao_hbm, wcat.at[0:width]),
        (fo_hbm, wcat.at[width : 2 * width]),
    ]
    copies = [
        pltpu.make_async_copy(src, dst, load_sem.at[i]) for i, (src, dst) in enumerate(loads)
    ]
    for copy in copies:
        copy.start()

    barrier = pltpu.get_barrier_semaphore()
    for neighbour in (left, right):
        pl.semaphore_signal(barrier, inc=1, device_id={"sp": neighbour}, device_id_type=MESH)
    for r in range(1, tps):
        pl.semaphore_signal(
            barrier, inc=1, device_id={"tp": lax.rem(tp + r, tps)}, device_id_type=MESH
        )

    half = rows // 2

    def pieces(slot):
        return [
            obuf.at[slot],
            kbuf.at[slot, pl.ds(0, half)],
            kbuf.at[slot, pl.ds(half, half)],
            vbuf.at[slot, pl.ds(0, half)],
            vbuf.at[slot, pl.ds(half, half)],
        ]

    def hop(slot, step, plus):
        ssem, rsem = (plus_send, plus_recv) if plus else (minus_send, minus_recv)
        to = right if plus else left
        return [
            pltpu.make_async_remote_copy(
                src_ref=piece,
                dst_ref=piece,
                send_sem=ssem.at[step, i],
                recv_sem=rsem.at[step, i],
                device_id={"sp": to},
                device_id_type=MESH,
            )
            for i, piece in enumerate(pieces(slot))
        ]

    def plus_sends(step):
        return (me - step >= 0) & (me < n - 1) & (step < dist)

    def minus_gets(device, step):
        block = lax.rem(device + step, n)
        return (step < dist) & (block <= low) & ((device < block) | (device > block + dist))

    def minus_sends(step):
        block = lax.rem(me + step, n)
        fits = (step == 0) | minus_gets(me, step)
        return fits & (block <= low) & minus_gets(left, step + 1)

    row_id = lax.broadcasted_iota(jnp.int32, (rows, rows), 0)
    col_id = lax.broadcasted_iota(jnp.int32, (rows, rows), 1)
    tri[...] = (row_id > col_id).astype(f32).astype(bf16)
    offsets = off_ref[...].astype(f32)
    padded = jnp.concatenate([offsets, jnp.zeros((rows, 126), f32)], axis=1)
    obuf[me] = padded.T[0:2].astype(bf16)

    gain = gain_ref[...].astype(f32).reshape(1, gain_ref.shape[0])
    copies[0].wait()

    @pl.loop(0, rows // 32)
    def _(i):
        at = pl.ds(pl.multiple_of(i * 32, 32), 32)
        xf = x_v[at].astype(f32)
        scale = lax.rsqrt(jnp.mean(xf * xf, axis=-1, keepdims=True) + rms_eps)
        normed[at] = (xf * scale * gain).astype(bf16)

    copies[1].wait()
    copies[2].wait()
    kv = jnp.dot(normed[...], w_v[:, 0 : 2 * width], preferred_element_type=f32)
    kbuf[me] = kv[:, 0:width].astype(bf16)
    vbuf[me] = kv[:, width : 2 * width].astype(bf16)

    pl.semaphore_wait(barrier, tps + 1)

    @pl.when(plus_sends(0))
    def _():
        for copy in hop(me, 0, True):
            copy.start()

    @pl.when(minus_sends(0))
    def _():
        for copy in hop(me, 0, False):
            copy.start()

    for i in (3, 4, 5):
        copies[i].wait()
    qig = jnp.dot(normed[...], w_v[:, 2 * width : 5 * width], preferred_element_type=f32)
    gate = qig[:, 2 * width : 3 * width].astype(bf16).astype(f32)
    conv_in = qig[:, width : 2 * width].astype(bf16).astype(f32)
    gated_rows = (conv_in * (1.0 / (1.0 + jnp.exp(-gate)))).astype(bf16)
    gated[...] = gated_rows
    tail = 32
    halo_copy = pltpu.make_async_remote_copy(
        src_ref=gated.at[pl.ds(rows - tail, tail)],
        dst_ref=halo,
        send_sem=halo_sem.at[0],
        recv_sem=halo_sem.at[1],
        device_id={"sp": right},
        device_id_type=MESH,
    )

    @pl.when(me < n - 1)
    def _():
        halo_copy.start()

    lane = lax.broadcasted_iota(jnp.int32, (rows, width), 1)
    first = lane < HEAD_DIM
    query = qig[:, 0:width].astype(bf16).astype(f32) * HEAD_DIM ** (-0.5)
    qs[0:rows] = jnp.where(first, query, 0.0).astype(bf16)
    qs[rows : 2 * rows] = jnp.where(first, 0.0, query).astype(bf16)

    def attend(slot, chunk, strict):
        head = chunk * half // rows
        at = pl.ds(chunk * half, half)
        scores = dot_nt(qs[at], kbuf[slot]) + obuf[slot].astype(f32)[head : head + 1]
        soft = jnp.maximum(scores, 0.0) + jnp.log(1.0 + jnp.exp(-jnp.abs(scores)))
        gain_log = scores - soft
        if strict is not None:
            soft = jnp.where(strict, soft, 0.0)
        beyond = jnp.dot(soft.astype(bf16), tri[...], preferred_element_type=f32)
        weights = jnp.exp(gain_log - beyond)
        if strict is not None:
            weights = jnp.where(strict, weights, 0.0)
        part_sum = jnp.dot(weights.astype(bf16), vbuf[slot], preferred_element_type=f32)
        lost = jnp.broadcast_to(beyond[:, 0:1] + soft[:, 0:1], (half, width))
        return at, part_sum, lost

    chunks = 2 * rows // half
    for chunk in range(chunks):
        base = chunk * half % rows
        query_pos = lax.broadcasted_iota(jnp.int32, (half, rows), 0) + base
        key_pos = lax.broadcasted_iota(jnp.int32, (half, rows), 1)
        at, part_sum, lost = attend(me, chunk, key_pos < query_pos)
        acc_r[at] = part_sum
        sum_r[at] = lost
    acc_l[...] = jnp.zeros_like(acc_l)
    sum_l[...] = jnp.zeros_like(sum_l)

    stat_copies = [
        pltpu.make_async_remote_copy(
            src_ref=stat_send,
            dst_ref=stat_recv.at[r],
            send_sem=stat_ssem.at[r],
            recv_sem=stat_rsem.at[r],
            device_id={"tp": lax.rem(tp + r, tps)},
            device_id_type=MESH,
        )
        for r in range(1, tps)
    ]

    def convolve():
        @pl.when(me > 0)
        def _():
            halo_copy.wait_recv()
            ext[0:tail] = halo[...].astype(f32)

        @pl.when(me == 0)
        def _():
            ext[0:tail] = jnp.zeros((tail, width), f32)

        ext[tail : tail + rows] = gated[...].astype(f32)
        taps = taps_ref[...].astype(f32)
        for base in range(0, rows, half):
            total = jnp.zeros((half, width), f32)
            for k in range(reach + 1):
                total = total + ext[base + tail - reach + k : base + tail - reach + k + half] * taps[k : k + 1]
            filt[base : base + half] = total
        filtered = filt[...]
        sums = jnp.sum(filtered, axis=-1, keepdims=True)
        squares = jnp.sum(filtered * filtered, axis=-1, keepdims=True)
        both = jnp.where(lane == 0, sums, squares)
        stat_send[...] = both.T[0:8]
        for copy in stat_copies:
            copy.start()

    def normalize():
        total = stat_send[...]
        for r, copy in enumerate(stat_copies):
            copy.wait()
            total = total + stat_recv[r + 1]
        mean = total / (width * tps)
        center = mean[0:1]
        spread = jnp.maximum(mean[1:2] - center * center, 0.0)
        scale = lax.rsqrt(spread + norm_eps)
        line = lax.broadcasted_iota(jnp.int32, (width, rows), 0)
        columns = jnp.where(line == 0, center, scale).T
        hidden = (filt[...] - columns[:, 0:1]) * columns[:, 1:2]
        hidden = hidden * cgain_ref[...].astype(f32).reshape(1, width)
        hidden = hidden + cshift_ref[...].astype(f32).reshape(1, width)
        cat[:, width : 2 * width] = (hidden * (1.0 / (1.0 + jnp.exp(-hidden)))).astype(bf16)

    @pl.loop(1, dist + 1)
    def _(step):
        plus_block = me - step
        minus_block = lax.rem(me + step, n)
        got_plus = plus_block >= 0
        got_minus = minus_gets(me, step)

        @pl.when(got_plus)
        def _():
            arrived = hop(plus_block, step - 1, True)
            onward = hop(plus_block, step, True)
            for copy, ahead in zip(arrived, onward):
                copy.wait_recv()

                @pl.when(plus_sends(step))
                def _():
                    ahead.start()

        @pl.when(got_minus)
        def _():
            arrived = hop(minus_block, step - 1, False)
            onward = hop(minus_block, step, False)
            for copy, ahead in zip(arrived, onward):
                copy.wait_recv()

                @pl.when(minus_sends(step))
                def _():
                    ahead.start()

        @pl.when(got_plus)
        def _():
            for chunk in range(chunks):
                at, part_sum, lost = attend(plus_block, chunk, None)
                seen = sum_r[at]
                acc_r[at] = acc_r[at] + jnp.exp(-seen) * part_sum
                sum_r[at] = seen + lost

        @pl.when(got_minus & (me > minus_block))
        def _():
            for chunk in range(chunks):
                at, part_sum, lost = attend(minus_block, chunk, None)
                acc_l[at] = part_sum + jnp.exp(-lost) * acc_l[at]
                sum_l[at] = sum_l[at] + lost

        @pl.when(step == 1)
        def _():
            convolve()

        @pl.when(step == min(3, dist))
        def _():
            normalize()

    attended = acc_r[...] + jnp.exp(-sum_r[...]) * acc_l[...]
    lost = sum_r[...] + sum_l[...]
    mass = jnp.log(jnp.maximum(1.0 - jnp.exp(-lost), mass_floor))
    mass_ref[:, 0:1] = mass[0:rows, 0:1]
    mass_ref[:, 1:2] = mass[rows : 2 * rows, 0:1]
    attended = jnp.where(first, attended[0:rows], attended[rows : 2 * rows])
    power = attended * attended
    low_mean = jnp.sum(jnp.where(first, power, 0.0), axis=-1, keepdims=True) / HEAD_DIM
    high_mean = jnp.sum(jnp.where(first, 0.0, power), axis=-1, keepdims=True) / HEAD_DIM
    scale = jnp.where(first, lax.rsqrt(low_mean + rms_eps), lax.rsqrt(high_mean + rms_eps))
    heads = attended * scale * head_gain_ref[...].astype(f32).reshape(1, width)
    cat[:, 0:width] = heads.astype(bf16)

    copies[6].wait()
    copies[7].wait()
    features = wcat.shape[1]
    share = rows // tps
    tiles = 4
    span = features // tiles

    def exchange(tile, r):
        peer = lax.rem(tp + r, tps)
        columns = pl.ds(tile * span, span)
        return pltpu.make_async_remote_copy(
            src_ref=part.at[peer, :, columns],
            dst_ref=recv.at[r, :, columns],
            send_sem=rs_ssem.at[tile, r],
            recv_sem=rs_rsem.at[tile, r],
            device_id={"tp": peer},
            device_id_type=MESH,
        )

    for tile in range(tiles):
        columns = slice(tile * span, (tile + 1) * span)
        product = jnp.dot(cat[...], wcat[:, columns], preferred_element_type=f32).astype(bf16)
        part[:, :, columns] = product.reshape(tps, share, span)
        for r in range(1, tps):
            exchange(tile, r).start()
    for tile in range(tiles):
        columns = slice(tile * span, (tile + 1) * span)
        total = part[tp, :, columns].astype(f32)
        for r in range(1, tps):
            exchange(tile, r).wait()
            total = total + recv[r, :, columns].astype(f32)
        out_ref[:, columns] = total.astype(bf16)

    @pl.when(me < n - 1)
    def _():
        halo_copy.wait_send()

    @pl.loop(0, dist)
    def _(step):
        @pl.when(plus_sends(step))
        def _():
            for copy in hop(me - step, step, True):
                copy.wait_send()

        @pl.when(minus_sends(step))
        def _():
            for copy in hop(lax.rem(me + step, n), step, False):
                copy.wait_send()


def local(n, tps, stream, norm_gain, wq, wk, wv, wi, wg, offset, head_gain, taps, cgain, cshift, ao, fo):
    rows, features = stream.shape[1:]
    width = wq.shape[1]
    dist = n // 2
    dma = pltpu.SemaphoreType.DMA
    vmem = pl.BlockSpec(memory_space=pltpu.VMEM)
    anywhere = pl.BlockSpec(memory_space=pl.ANY)
    mixed, mass = pl.pallas_call(
        functools.partial(kernel, n, tps),
        out_shape=(
            jax.ShapeDtypeStruct((rows // tps, features), bf16),
            jax.ShapeDtypeStruct((rows, 2), f32),
        ),
        in_specs=[anywhere, vmem, anywhere, anywhere, anywhere, anywhere, anywhere]
        + [vmem] * 5
        + [anywhere, anywhere],
        out_specs=(vmem, vmem),
        scratch_shapes=[
            pltpu.VMEM((rows, features), bf16),
            pltpu.VMEM((rows, features), bf16),
            pltpu.VMEM((features, 5 * width), bf16),
            pltpu.VMEM((2 * width, features), bf16),
            pltpu.VMEM((n, rows, width), bf16),
            pltpu.VMEM((n, rows, width), bf16),
            pltpu.VMEM((n, 2, rows), bf16),
            pltpu.VMEM((2 * rows, width), bf16),
            pltpu.VMEM((rows, rows), bf16),
            pltpu.VMEM((2 * rows, width), f32),
            pltpu.VMEM((2 * rows, width), f32),
            pltpu.VMEM((2 * rows, width), f32),
            pltpu.VMEM((2 * rows, width), f32),
            pltpu.VMEM((rows, width), bf16),
            pltpu.VMEM((32, width), bf16),
            pltpu.VMEM((rows + 32, width), f32),
            pltpu.VMEM((rows, width), f32),
            pltpu.VMEM((8, rows), f32),
            pltpu.VMEM((tps, 8, rows), f32),
            pltpu.VMEM((rows, 2 * width), bf16),
            pltpu.VMEM((tps, rows // tps, features), bf16),
            pltpu.VMEM((tps, rows // tps, features), bf16),
            dma((8,)),
            dma((dist, 5)),
            dma((dist, 5)),
            dma((dist, 5)),
            dma((dist, 5)),
            dma((2,)),
            dma((tps,)),
            dma((tps,)),
            dma((4, tps)),
            dma((4, tps)),
        ],
        compiler_params=pltpu.CompilerParams(
            collective_id=0, has_side_effects=True, vmem_limit_bytes=48 * 1024 * 1024
        ),
        name="layer",
    )(stream[0], norm_gain, wq, wk, wv, wi, wg, offset[0], head_gain, taps, cgain, cshift, ao, fo)
    return mixed[None], mass[None]


def solution(mesh):
    return jax.shard_map(
        functools.partial(local, mesh.shape["sp"], mesh.shape["tp"]),
        mesh=mesh,
        in_specs=(
            P("fs", "sp", None),
            P(),
            P(None, "tp"),
            P(None, "tp"),
            P(None, "tp"),
            P(None, "tp"),
            P(None, "tp"),
            P("fs", "sp", "tp"),
            P("tp"),
            P(None, "tp"),
            P("tp"),
            P("tp"),
            P("tp", None),
            P("tp", None),
        ),
        out_specs=(P("fs", ("sp", "tp"), None), P("fs", "sp", "tp")),
        check_vma=False,
    )
```

```python
import functools

import jax
import jax.numpy as jnp
from jax import lax
from jax.experimental import pallas as pl
from jax.experimental.pallas import tpu as pltpu
from jax.sharding import PartitionSpec as P

HEAD_DIM = 64

rms_eps = 1e-06
norm_eps = 1e-05
mass_floor = 0.01

MESH = pl.DeviceIdType.MESH
f32 = jnp.float32
bf16 = jnp.bfloat16


def dot_nt(a, b):
    return lax.dot_general(a, b, (((1,), (1,)), ((), ())), preferred_element_type=f32)


def kernel(
    n,
    tps,
    x_hbm,
    gain_hbm,
    wq_hbm,
    wk_hbm,
    wv_hbm,
    wi_hbm,
    wg_hbm,
    off_hbm,
    head_gain_hbm,
    taps_hbm,
    cgain_hbm,
    cshift_hbm,
    ao_hbm,
    fo_hbm,
    out_ref,
    mass_ref,
    x_v,
    gain_ref,
    head_gain_ref,
    taps_ref,
    cgain_ref,
    cshift_ref,
    normed,
    w_v,
    wcat,
    kbuf,
    vbuf,
    obuf,
    qs,
    tri,
    acc_r,
    sum_r,
    acc_l,
    sum_l,
    gated,
    halo,
    ext,
    filt,
    stat_send,
    stat_recv,
    cat,
    part,
    recv,
    load_sem,
    plus_send,
    plus_recv,
    minus_send,
    minus_recv,
    halo_sem,
    stat_ssem,
    stat_rsem,
    rs_ssem,
    rs_rsem,
):
    rows = x_hbm.shape[0]
    width = wq_hbm.shape[1]
    reach = taps_ref.shape[0] - 1
    me = lax.axis_index("sp")
    tp = lax.axis_index("tp")
    right = lax.rem(me + 1, n)
    left = lax.rem(me + n - 1, n)
    dist = n // 2
    low = n - dist - 2

    loads = [
        (x_hbm, x_v),
        (gain_hbm, gain_ref),
        (off_hbm, obuf.at[me]),
        (wk_hbm, w_v.at[:, 0:width]),
        (wv_hbm, w_v.at[:, width : 2 * width]),
        (wq_hbm, w_v.at[:, 2 * width : 3 * width]),
        (wi_hbm, w_v.at[:, 3 * width : 4 * width]),
        (wg_hbm, w_v.at[:, 4 * width : 5 * width]),
        (ao_hbm, wcat.at[0:width]),
        (fo_hbm, wcat.at[width : 2 * width]),
        (taps_hbm, taps_ref),
        (head_gain_hbm, head_gain_ref),
        (cgain_hbm, cgain_ref),
        (cshift_hbm, cshift_ref),
    ]
    copies = [
        pltpu.make_async_copy(src, dst, load_sem.at[i]) for i, (src, dst) in enumerate(loads)
    ]
    for copy in copies[0:5]:
        copy.start()

    barrier = pltpu.get_barrier_semaphore()
    for neighbour in (left, right):
        pl.semaphore_signal(barrier, inc=1, device_id={"sp": neighbour}, device_id_type=MESH)
    for r in range(1, tps):
        pl.semaphore_signal(
            barrier, inc=1, device_id={"tp": lax.rem(tp + r, tps)}, device_id_type=MESH
        )

    half = rows // 2

    def pieces(slot):
        return [
            obuf.at[slot],
            kbuf.at[slot, pl.ds(0, half)],
            kbuf.at[slot, pl.ds(half, half)],
            vbuf.at[slot, pl.ds(0, half)],
            vbuf.at[slot, pl.ds(half, half)],
        ]

    def hop(slot, step, plus):
        ssem, rsem = (plus_send, plus_recv) if plus else (minus_send, minus_recv)
        to = right if plus else left
        return [
            pltpu.make_async_remote_copy(
                src_ref=piece,
                dst_ref=piece,
                send_sem=ssem.at[step, i],
                recv_sem=rsem.at[step, i],
                device_id={"sp": to},
                device_id_type=MESH,
            )
            for i, piece in enumerate(pieces(slot))
        ]

    def plus_sends(step):
        return (me - step >= 0) & (me < n - 1) & (step < dist)

    def minus_gets(device, step):
        block = lax.rem(device + step, n)
        return (step < dist) & (block <= low) & ((device < block) | (device > block + dist))

    def minus_sends(step):
        block = lax.rem(me + step, n)
        fits = (step == 0) | minus_gets(me, step)
        return fits & (block <= low) & minus_gets(left, step + 1)

    row_id = lax.broadcasted_iota(jnp.int32, (rows, rows), 0)
    col_id = lax.broadcasted_iota(jnp.int32, (rows, rows), 1)
    tri[...] = (row_id > col_id).astype(f32).astype(bf16)

    copies[1].wait()
    gain = gain_ref[...].astype(f32).reshape(1, gain_ref.shape[0])
    copies[0].wait()
    for copy in copies[5:]:
        copy.start()

    @pl.loop(0, rows // 32)
    def _(i):
        at = pl.ds(pl.multiple_of(i * 32, 32), 32)
        xf = x_v[at].astype(f32)
        scale = lax.rsqrt(jnp.mean(xf * xf, axis=-1, keepdims=True) + rms_eps)
        normed[at] = (xf * scale * gain).astype(bf16)

    for i in (2, 3, 4):
        copies[i].wait()
    kv = jnp.dot(normed[...], w_v[:, 0 : 2 * width], preferred_element_type=f32)
    kbuf[me] = kv[:, 0:width].astype(bf16)
    vbuf[me] = kv[:, width : 2 * width].astype(bf16)

    pl.semaphore_wait(barrier, tps + 1)

    @pl.when(plus_sends(0))
    def _():
        for copy in hop(me, 0, True):
            copy.start()

    @pl.when(minus_sends(0))
    def _():
        for copy in hop(me, 0, False):
            copy.start()

    for i in (5, 6, 7):
        copies[i].wait()
    qig = jnp.dot(normed[...], w_v[:, 2 * width : 5 * width], preferred_element_type=f32)
    gate = qig[:, 2 * width : 3 * width].astype(bf16).astype(f32)
    conv_in = qig[:, width : 2 * width].astype(bf16).astype(f32)
    gated_rows = (conv_in * (1.0 / (1.0 + jnp.exp(-gate)))).astype(bf16)
    gated[...] = gated_rows
    tail = 32
    halo_copy = pltpu.make_async_remote_copy(
        src_ref=gated.at[pl.ds(rows - tail, tail)],
        dst_ref=halo,
        send_sem=halo_sem.at[0],
        recv_sem=halo_sem.at[1],
        device_id={"sp": right},
        device_id_type=MESH,
    )

    @pl.when(me < n - 1)
    def _():
        halo_copy.start()

    lane = lax.broadcasted_iota(jnp.int32, (rows, width), 1)
    first = lane < HEAD_DIM
    query = qig[:, 0:width].astype(bf16).astype(f32) * HEAD_DIM ** (-0.5)
    qs[0:rows] = jnp.where(first, query, 0.0).astype(bf16)
    qs[rows : 2 * rows] = jnp.where(first, 0.0, query).astype(bf16)

    def attend(slot, chunk, strict):
        head = chunk * half // rows
        at = pl.ds(chunk * half, half)
        scores = dot_nt(qs[at], kbuf[slot]) + obuf[slot].astype(f32)[head : head + 1]
        soft = jnp.maximum(scores, 0.0) + jnp.log(1.0 + jnp.exp(-jnp.abs(scores)))
        gain_log = scores - soft
        if strict is not None:
            soft = jnp.where(strict, soft, 0.0)
        beyond = jnp.dot(soft.astype(bf16), tri[...], preferred_element_type=f32)
        weights = jnp.exp(gain_log - beyond)
        if strict is not None:
            weights = jnp.where(strict, weights, 0.0)
        part_sum = jnp.dot(weights.astype(bf16), vbuf[slot], preferred_element_type=f32)
        lost = jnp.broadcast_to(beyond[:, 0:1] + soft[:, 0:1], (half, width))
        return at, part_sum, lost

    chunks = 2 * rows // half
    for chunk in range(chunks):
        base = chunk * half % rows
        query_pos = lax.broadcasted_iota(jnp.int32, (half, rows), 0) + base
        key_pos = lax.broadcasted_iota(jnp.int32, (half, rows), 1)
        at, part_sum, lost = attend(me, chunk, key_pos < query_pos)
        acc_r[at] = part_sum
        sum_r[at] = lost
    for i in (10, 11, 12, 13):
        copies[i].wait()
    acc_l[...] = jnp.zeros_like(acc_l)
    sum_l[...] = jnp.zeros_like(sum_l)

    stat_copies = [
        pltpu.make_async_remote_copy(
            src_ref=stat_send,
            dst_ref=stat_recv.at[r],
            send_sem=stat_ssem.at[r],
            recv_sem=stat_rsem.at[r],
            device_id={"tp": lax.rem(tp + r, tps)},
            device_id_type=MESH,
        )
        for r in range(1, tps)
    ]

    def convolve():
        @pl.when(me > 0)
        def _():
            halo_copy.wait_recv()
            ext[0:tail] = halo[...].astype(f32)

        @pl.when(me == 0)
        def _():
            ext[0:tail] = jnp.zeros((tail, width), f32)

        ext[tail : tail + rows] = gated[...].astype(f32)
        taps = taps_ref[...].astype(f32)
        for base in range(0, rows, half):
            total = jnp.zeros((half, width), f32)
            for k in range(reach + 1):
                total = total + ext[base + tail - reach + k : base + tail - reach + k + half] * taps[k : k + 1]
            filt[base : base + half] = total
        filtered = filt[...]
        sums = jnp.sum(filtered, axis=-1, keepdims=True)
        squares = jnp.sum(filtered * filtered, axis=-1, keepdims=True)
        both = jnp.where(lane == 0, sums, squares)
        stat_send[...] = both.T[0:8]
        for copy in stat_copies:
            copy.start()

    def normalize():
        total = stat_send[...]
        for r, copy in enumerate(stat_copies):
            copy.wait()
            total = total + stat_recv[r + 1]
        mean = total / (width * tps)
        center = mean[0:1]
        spread = jnp.maximum(mean[1:2] - center * center, 0.0)
        scale = lax.rsqrt(spread + norm_eps)
        line = lax.broadcasted_iota(jnp.int32, (width, rows), 0)
        columns = jnp.where(line == 0, center, scale).T
        hidden = (filt[...] - columns[:, 0:1]) * columns[:, 1:2]
        hidden = hidden * cgain_ref[...].astype(f32).reshape(1, width)
        hidden = hidden + cshift_ref[...].astype(f32).reshape(1, width)
        cat[:, width : 2 * width] = (hidden * (1.0 / (1.0 + jnp.exp(-hidden)))).astype(bf16)

    features = wcat.shape[1]
    share = rows // tps
    tiles = 4
    span = features // tiles

    def exchange(tile, r):
        peer = lax.rem(tp + r, tps)
        columns = pl.ds(tile * span, span)
        return pltpu.make_async_remote_copy(
            src_ref=part.at[peer, :, columns],
            dst_ref=recv.at[r, :, columns],
            send_sem=rs_ssem.at[tile, r],
            recv_sem=rs_rsem.at[tile, r],
            device_id={"tp": peer},
            device_id_type=MESH,
        )

    def finish():
        attended = acc_r[...] + jnp.exp(-sum_r[...]) * acc_l[...]
        lost = sum_r[...] + sum_l[...]
        mass = jnp.log(jnp.maximum(1.0 - jnp.exp(-jnp.where(first, lost[0:rows], lost[rows : 2 * rows])), mass_floor)).T
        mass_ref[0:1] = mass[0:1]
        mass_ref[1:2] = mass[HEAD_DIM : HEAD_DIM + 1]
        attended = jnp.where(first, attended[0:rows], attended[rows : 2 * rows])
        power = attended * attended
        low_mean = jnp.sum(jnp.where(first, power, 0.0), axis=-1, keepdims=True) / HEAD_DIM
        high_mean = jnp.sum(jnp.where(first, 0.0, power), axis=-1, keepdims=True) / HEAD_DIM
        scale = jnp.where(first, lax.rsqrt(low_mean + rms_eps), lax.rsqrt(high_mean + rms_eps))
        heads = attended * scale * head_gain_ref[...].astype(f32).reshape(1, width)
        cat[:, 0:width] = heads.astype(bf16)

        copies[8].wait()
        copies[9].wait()
        for tile in range(tiles):
            columns = slice(tile * span, (tile + 1) * span)
            product = jnp.dot(cat[...], wcat[:, columns], preferred_element_type=f32).astype(bf16)
            part[:, :, columns] = product.reshape(tps, share, span)
            for r in range(1, tps):
                exchange(tile, r).start()

    @pl.loop(1, dist + 2)
    def _(step):
        plus_block = me - step
        minus_block = lax.rem(me + step, n)
        got_plus = (plus_block >= 0) & (step <= dist)
        got_minus = minus_gets(me, step)
        past_plus = plus_block + 1
        past_minus = lax.rem(me + step - 1, n)
        has_plus = (past_plus >= 0) & (step > 1)
        has_minus = minus_gets(me, step - 1) & (step > 1) & (me > past_minus)
        plus_arrived = hop(plus_block, step - 1, True)
        plus_onward = hop(plus_block, step, True)
        minus_arrived = hop(minus_block, step - 1, False)
        minus_onward = hop(minus_block, step, False)

        for i in range(chunks + 1):

            @pl.when(got_plus)
            def _():
                plus_arrived[i].wait_recv()

            @pl.when(got_plus & plus_sends(step))
            def _():
                plus_onward[i].start()

            @pl.when(got_minus)
            def _():
                minus_arrived[i].wait_recv()

            @pl.when(got_minus & minus_sends(step))
            def _():
                minus_onward[i].start()

            if i == 0:
                continue
            chunk = i - 1

            @pl.when(has_plus)
            def _():
                at, part_sum, lost = attend(past_plus, chunk, None)
                seen = sum_r[at]
                acc_r[at] = acc_r[at] + jnp.exp(-seen) * part_sum
                sum_r[at] = seen + lost

            @pl.when(has_minus)
            def _():
                at, part_sum, lost = attend(past_minus, chunk, None)
                acc_l[at] = part_sum + jnp.exp(-lost) * acc_l[at]
                sum_l[at] = sum_l[at] + lost

        @pl.when(step == 1)
        def _():
            convolve()

        @pl.when(step == min(3, dist))
        def _():
            normalize()

        @pl.when(step == jnp.clip(me + 1, min(3, dist), dist + 1))
        def _():
            finish()

    for tile in range(tiles):
        columns = slice(tile * span, (tile + 1) * span)
        total = part[tp, :, columns].astype(f32)
        for r in range(1, tps):
            exchange(tile, r).wait()
            total = total + recv[r, :, columns].astype(f32)
        out_ref[:, columns] = total.astype(bf16)

    @pl.when(me < n - 1)
    def _():
        halo_copy.wait_send()

    @pl.loop(0, dist)
    def _(step):
        @pl.when(plus_sends(step))
        def _():
            for copy in hop(me - step, step, True):
                copy.wait_send()

        @pl.when(minus_sends(step))
        def _():
            for copy in hop(lax.rem(me + step, n), step, False):
                copy.wait_send()


def local(n, tps, stream, norm_gain, wq, wk, wv, wi, wg, offset, head_gain, taps, cgain, cshift, ao, fo):
    rows, features = stream.shape[1:]
    width = wq.shape[1]
    dist = n // 2
    dma = pltpu.SemaphoreType.DMA
    vmem = pl.BlockSpec(memory_space=pltpu.VMEM)
    anywhere = pl.BlockSpec(memory_space=pltpu.HBM)
    mixed, mass = pl.pallas_call(
        functools.partial(kernel, n, tps),
        out_shape=(
            jax.ShapeDtypeStruct((rows // tps, features), bf16),
            jax.ShapeDtypeStruct((2, rows), f32),
        ),
        in_specs=[anywhere] * 14,
        out_specs=(vmem, vmem),
        scratch_shapes=[
            pltpu.VMEM((rows, features), bf16),
            pltpu.VMEM((features,), bf16),
            pltpu.VMEM((width,), bf16),
            pltpu.VMEM(taps.shape, bf16),
            pltpu.VMEM((width,), bf16),
            pltpu.VMEM((width,), bf16),
            pltpu.VMEM((rows, features), bf16),
            pltpu.VMEM((features, 5 * width), bf16),
            pltpu.VMEM((2 * width, features), bf16),
            pltpu.VMEM((n, rows, width), bf16),
            pltpu.VMEM((n, rows, width), bf16),
            pltpu.VMEM((n, 2, rows), bf16),
            pltpu.VMEM((2 * rows, width), bf16),
            pltpu.VMEM((rows, rows), bf16),
            pltpu.VMEM((2 * rows, width), f32),
            pltpu.VMEM((2 * rows, width), f32),
            pltpu.VMEM((2 * rows, width), f32),
            pltpu.VMEM((2 * rows, width), f32),
            pltpu.VMEM((rows, width), bf16),
            pltpu.VMEM((32, width), bf16),
            pltpu.VMEM((rows + 32, width), f32),
            pltpu.VMEM((rows, width), f32),
            pltpu.VMEM((8, rows), f32),
            pltpu.VMEM((tps, 8, rows), f32),
            pltpu.VMEM((rows, 2 * width), bf16),
            pltpu.VMEM((tps, rows // tps, features), bf16),
            pltpu.VMEM((tps, rows // tps, features), bf16),
            dma((14,)),
            dma((dist, 5)),
            dma((dist, 5)),
            dma((dist, 5)),
            dma((dist, 5)),
            dma((2,)),
            dma((tps,)),
            dma((tps,)),
            dma((4, tps)),
            dma((4, tps)),
        ],
        compiler_params=pltpu.CompilerParams(
            collective_id=0, has_side_effects=True, vmem_limit_bytes=48000000
        ),
        name="layer",
    )(*[pltpu.with_memory_space_constraint(a, pltpu.HBM) for a in (stream[0], norm_gain, wq, wk, wv, wi, wg, offset[0].T, head_gain, taps, cgain, cshift, ao, fo)])
    return mixed[None], mass.T[None]


def solution(mesh):
    return jax.shard_map(
        functools.partial(local, mesh.shape["sp"], mesh.shape["tp"]),
        mesh=mesh,
        in_specs=(
            P("fs", "sp", None),
            P(),
            P(None, "tp"),
            P(None, "tp"),
            P(None, "tp"),
            P(None, "tp"),
            P(None, "tp"),
            P("fs", "sp", "tp"),
            P("tp"),
            P(None, "tp"),
            P("tp"),
            P("tp"),
            P("tp", None),
            P("tp", None),
        ),
        out_specs=(P("fs", ("sp", "tp"), None), P("fs", "sp", "tp")),
        check_vma=False,
    )
```

```python
import functools

import jax
import jax.numpy as jnp
from jax import lax
from jax.experimental import pallas as pl
from jax.experimental.pallas import tpu as pltpu
from jax.sharding import PartitionSpec as P

HEAD_DIM = 64

rms_eps = 1e-06
norm_eps = 1e-05
mass_floor = 0.01

MESH = pl.DeviceIdType.MESH
f32 = jnp.float32
bf16 = jnp.bfloat16


def dot_nt(a, b):
    return lax.dot_general(a, b, (((1,), (1,)), ((), ())), preferred_element_type=f32)


def kernel(
    n,
    tps,
    x_hbm,
    gain_hbm,
    wq_hbm,
    wk_hbm,
    wv_hbm,
    wi_hbm,
    wg_hbm,
    off_hbm,
    head_gain_hbm,
    taps_hbm,
    cgain_hbm,
    cshift_hbm,
    ao_hbm,
    fo_hbm,
    out_ref,
    mass_ref,
    x_v,
    gain_ref,
    head_gain_ref,
    taps_ref,
    cgain_ref,
    cshift_ref,
    normed,
    w_v,
    wa,
    fo_v,
    kbuf,
    vbuf,
    obuf,
    qs,
    tri,
    acc_r,
    sum_r,
    acc_l,
    sum_l,
    gated,
    halo,
    ext,
    filt,
    stat_send,
    stat_recv,
    conv_v,
    part,
    pair,
    both,
    recv,
    conv_sum,
    head_send,
    head_recv,
    load_sem,
    plus_send,
    plus_recv,
    minus_send,
    minus_recv,
    halo_sem,
    stat_ssem,
    stat_rsem,
    pair_sem,
    rs_ssem,
    rs_rsem,
    gather_ssem,
    gather_rsem,
    head_ssem,
    head_rsem,
):
    rows = x_hbm.shape[0]
    width = wq_hbm.shape[1]
    reach = taps_ref.shape[0] - 1
    me = lax.axis_index("sp")
    tp = lax.axis_index("tp")
    right = lax.rem(me + 1, n)
    left = lax.rem(me + n - 1, n)
    dist = n // 2
    low = n - dist - 2

    def rows_of(device):
        return pl.ds(pl.multiple_of(device * width, width), width)

    loads = [
        (x_hbm, x_v),
        (gain_hbm, gain_ref),
        (off_hbm, obuf.at[me]),
        (wk_hbm, w_v.at[:, 0:width]),
        (wv_hbm, w_v.at[:, width : 2 * width]),
        (wq_hbm, w_v.at[:, 2 * width : 3 * width]),
        (wi_hbm, w_v.at[:, 3 * width : 4 * width]),
        (wg_hbm, w_v.at[:, 4 * width : 5 * width]),
        (ao_hbm, wa.at[rows_of(tp)]),
        (fo_hbm, fo_v),
        (taps_hbm, taps_ref),
        (head_gain_hbm, head_gain_ref),
        (cgain_hbm, cgain_ref),
        (cshift_hbm, cshift_ref),
    ]
    copies = [
        pltpu.make_async_copy(src, dst, load_sem.at[i]) for i, (src, dst) in enumerate(loads)
    ]
    for copy in copies[0:5]:
        copy.start()

    barrier = pltpu.get_barrier_semaphore()
    for neighbour in (left, right):
        pl.semaphore_signal(barrier, inc=1, device_id={"sp": neighbour}, device_id_type=MESH)
    for r in range(1, tps):
        pl.semaphore_signal(
            barrier, inc=1, device_id={"tp": lax.rem(tp + r, tps)}, device_id_type=MESH
        )

    half = rows // 2

    def pieces(slot):
        quarters = [pl.ds(i * rows // 4, rows // 4) for i in range(4)]
        return (
            [obuf.at[slot]]
            + [kbuf.at[slot, quarter] for quarter in quarters]
            + [vbuf.at[slot, quarter] for quarter in quarters]
        )

    def hop(slot, step, plus):
        ssem, rsem = (plus_send, plus_recv) if plus else (minus_send, minus_recv)
        to = right if plus else left
        return [
            pltpu.make_async_remote_copy(
                src_ref=piece,
                dst_ref=piece,
                send_sem=ssem.at[step, i],
                recv_sem=rsem.at[step, i],
                device_id={"sp": to},
                device_id_type=MESH,
            )
            for i, piece in enumerate(pieces(slot))
        ]

    def plus_sends(step):
        return (me - step >= 0) & (me < n - 1) & (step < dist)

    def minus_gets(device, step):
        block = lax.rem(device + step, n)
        return (step < dist) & (block <= low) & ((device < block) | (device > block + dist))

    def minus_sends(step):
        block = lax.rem(me + step, n)
        fits = (step == 0) | minus_gets(me, step)
        return fits & (block <= low) & minus_gets(left, step + 1)

    row_id = lax.broadcasted_iota(jnp.int32, (rows, rows), 0)
    col_id = lax.broadcasted_iota(jnp.int32, (rows, rows), 1)
    tri[...] = (row_id > col_id).astype(f32).astype(bf16)

    copies[1].wait()
    gain = gain_ref[...].astype(f32).reshape(1, gain_ref.shape[0])
    copies[0].wait()
    for copy in copies[5:]:
        copy.start()

    @pl.loop(0, rows // 32)
    def _(i):
        at = pl.ds(pl.multiple_of(i * 32, 32), 32)
        xf = x_v[at].astype(f32)
        scale = lax.rsqrt(jnp.mean(xf * xf, axis=-1, keepdims=True) + rms_eps)
        normed[at] = (xf * scale * gain).astype(bf16)

    for i in (2, 3, 4):
        copies[i].wait()
    kv = jnp.dot(normed[...], w_v[:, 0 : 2 * width], preferred_element_type=f32)
    kbuf[me] = kv[:, 0:width].astype(bf16)
    vbuf[me] = kv[:, width : 2 * width].astype(bf16)

    pl.semaphore_wait(barrier, tps + 1)

    @pl.when(plus_sends(0))
    def _():
        for copy in hop(me, 0, True):
            copy.start()

    @pl.when(minus_sends(0))
    def _():
        for copy in hop(me, 0, False):
            copy.start()

    chips = tps // 2
    chip, core = tp // 2, lax.rem(tp, 2)
    sibling = tp + 1 - 2 * core
    ahead = 2 * lax.rem(chip + 1, chips) + core
    behind = 2 * lax.rem(chip + chips - 1, chips) + core
    across = 2 * lax.rem(chip + 2, chips) + core
    fold = width // 4

    def spread(i, device, to, start=0, size=width):
        part_rows = wa.at[pl.ds(pl.multiple_of(device * width + start, fold), size)]
        return pltpu.make_async_remote_copy(
            src_ref=part_rows,
            dst_ref=part_rows,
            send_sem=gather_ssem.at[i],
            recv_sem=gather_rsem.at[i],
            device_id={"tp": to},
            device_id_type=MESH,
        )

    def own_part(q):
        return (
            spread(q, tp, ahead, q * fold, fold),
            spread(4 + q, tp, behind, lax.rem(q + 2, 4) * fold, fold),
        )

    def onward_part(q):
        return (
            spread(8 + q, behind, ahead, q * fold, fold),
            spread(10 + q, ahead, behind, (q + 2) * fold, fold),
        )

    aside = [spread(12 + i, device, sibling) for i, device in enumerate((tp, behind, ahead, across))]
    copies[8].wait()
    for copy in own_part(0):
        copy.start()

    for i in (5, 6, 7):
        copies[i].wait()
    qig = jnp.dot(normed[...], w_v[:, 2 * width : 5 * width], preferred_element_type=f32)
    gate = qig[:, 2 * width : 3 * width].astype(bf16).astype(f32)
    conv_in = qig[:, width : 2 * width].astype(bf16).astype(f32)
    gated_rows = (conv_in * (1.0 / (1.0 + jnp.exp(-gate)))).astype(bf16)
    gated[...] = gated_rows
    tail = 32
    halo_copy = pltpu.make_async_remote_copy(
        src_ref=gated.at[pl.ds(rows - tail, tail)],
        dst_ref=halo,
        send_sem=halo_sem.at[0],
        recv_sem=halo_sem.at[1],
        device_id={"sp": right},
        device_id_type=MESH,
    )

    @pl.when(me < n - 1)
    def _():
        halo_copy.start()

    lane = lax.broadcasted_iota(jnp.int32, (rows, width), 1)
    first = lane < HEAD_DIM
    query = qig[:, 0:width].astype(bf16).astype(f32) * HEAD_DIM ** (-0.5)
    qs[0:rows] = jnp.where(first, query, 0.0).astype(bf16)
    qs[rows : 2 * rows] = jnp.where(first, 0.0, query).astype(bf16)

    def attend(slot, chunk, strict):
        head = chunk * half // rows
        at = pl.ds(chunk * half, half)
        scores = dot_nt(qs[at], kbuf[slot]) + obuf[slot].astype(f32)[head : head + 1]
        soft = jnp.maximum(jnp.log(1.0 + jnp.exp(jnp.minimum(scores, 80.0))), scores)
        gain_log = scores - soft
        if strict is not None:
            soft = jnp.where(strict, soft, 0.0)
        beyond = jnp.dot(soft.astype(bf16), tri[...], preferred_element_type=f32)
        weights = jnp.exp(gain_log - beyond)
        if strict is not None:
            weights = jnp.where(strict, weights, 0.0)
        part_sum = jnp.dot(weights.astype(bf16), vbuf[slot], preferred_element_type=f32)
        lost = jnp.broadcast_to(beyond[:, 0:1] + soft[:, 0:1], (half, width))
        return at, part_sum, lost

    chunks = 2 * rows // half
    for chunk in range(chunks):
        base = chunk * half % rows
        query_pos = lax.broadcasted_iota(jnp.int32, (half, rows), 0) + base
        key_pos = lax.broadcasted_iota(jnp.int32, (half, rows), 1)
        at, part_sum, lost = attend(me, chunk, key_pos < query_pos)
        acc_r[at] = part_sum
        sum_r[at] = lost
    for i in (10, 11, 12, 13):
        copies[i].wait()
    acc_l[...] = jnp.zeros_like(acc_l)
    sum_l[...] = jnp.zeros_like(sum_l)

    stat_copies = [
        pltpu.make_async_remote_copy(
            src_ref=stat_send,
            dst_ref=stat_recv.at[r],
            send_sem=stat_ssem.at[r],
            recv_sem=stat_rsem.at[r],
            device_id={"tp": lax.rem(tp + r, tps)},
            device_id_type=MESH,
        )
        for r in range(1, tps)
    ]

    def convolve():
        @pl.when(me > 0)
        def _():
            halo_copy.wait_recv()
            ext[0:tail] = halo[...].astype(f32)

        @pl.when(me == 0)
        def _():
            ext[0:tail] = jnp.zeros((tail, width), f32)

        ext[tail : tail + rows] = gated[...].astype(f32)

    def filter_rows(base):
        taps = taps_ref[...].astype(f32)
        total = jnp.zeros((half, width), f32)
        for k in range(reach + 1):
            total = total + ext[base + tail - reach + k : base + tail - reach + k + half] * taps[k : k + 1]
        filt[base : base + half] = total

    def statistics():
        filtered = filt[...]
        sums = jnp.sum(filtered, axis=-1, keepdims=True)
        squares = jnp.sum(filtered * filtered, axis=-1, keepdims=True)
        packed = jnp.where(lane == 0, sums, squares)
        stat_send[...] = packed.T[0:8]
        for copy in stat_copies:
            copy.start()

    def normalize():
        total = stat_send[...]
        for r, copy in enumerate(stat_copies):
            copy.wait()
            total = total + stat_recv[r + 1]
        mean = total / (width * tps)
        center = mean[0:1]
        spread = jnp.maximum(mean[1:2] - center * center, 0.0)
        scale = lax.rsqrt(spread + norm_eps)
        line = lax.broadcasted_iota(jnp.int32, (width, rows), 0)
        columns = jnp.where(line == 0, center, scale).T
        hidden = (filt[...] - columns[:, 0:1]) * columns[:, 1:2]
        hidden = hidden * cgain_ref[...].astype(f32).reshape(1, width)
        hidden = hidden + cshift_ref[...].astype(f32).reshape(1, width)
        conv_v[...] = (hidden * (1.0 / (1.0 + jnp.exp(-hidden)))).astype(bf16)
        copies[9].wait()

    features = wa.shape[1]
    share = rows // tps
    tiles = 4
    span = features // tiles

    def swap(tile):
        columns = pl.ds(tile * span, span)
        return pltpu.make_async_remote_copy(
            src_ref=part.at[:, 1 - core, :, columns],
            dst_ref=pair.at[:, :, columns],
            send_sem=pair_sem.at[0, tile],
            recv_sem=pair_sem.at[1, tile],
            device_id={"tp": sibling},
            device_id_type=MESH,
        )

    def exchange(tile, r):
        columns = pl.ds(tile * span, span)
        return pltpu.make_async_remote_copy(
            src_ref=both.at[r, :, columns],
            dst_ref=recv.at[r, :, columns],
            send_sem=rs_ssem.at[tile, r],
            recv_sem=rs_rsem.at[tile, r],
            device_id={"tp": 2 * lax.rem(chip + r, chips) + core},
            device_id_type=MESH,
        )

    def finish():
        attended = acc_r[...] + jnp.exp(-sum_r[...]) * acc_l[...]
        lost = sum_r[...] + sum_l[...]
        mass = jnp.log(jnp.maximum(1.0 - jnp.exp(-jnp.where(first, lost[0:rows], lost[rows : 2 * rows])), mass_floor)).T
        mass_ref[0:1] = mass[0:1]
        mass_ref[1:2] = mass[HEAD_DIM : HEAD_DIM + 1]
        attended = jnp.where(first, attended[0:rows], attended[rows : 2 * rows])
        power = attended * attended
        low_mean = jnp.sum(jnp.where(first, power, 0.0), axis=-1, keepdims=True) / HEAD_DIM
        high_mean = jnp.sum(jnp.where(first, 0.0, power), axis=-1, keepdims=True) / HEAD_DIM
        scale = jnp.where(first, lax.rsqrt(low_mean + rms_eps), lax.rsqrt(high_mean + rms_eps))
        heads = attended * scale * head_gain_ref[...].astype(f32).reshape(1, width)
        head_send[...] = heads.astype(bf16).reshape(tps, share, width)
        for r in range(1, tps):
            pass_heads(r).start()
        head_recv[tp] = head_send[tp]

    def pass_heads(r):
        peer = lax.rem(tp + r, tps)
        return pltpu.make_async_remote_copy(
            src_ref=head_send.at[peer],
            dst_ref=head_recv.at[tp],
            send_sem=head_ssem.at[r],
            recv_sem=head_rsem.at[r],
            device_id={"tp": peer},
            device_id_type=MESH,
        )

    def project(tile):
        columns = slice(tile * span, (tile + 1) * span)
        product = jnp.dot(conv_v[...], fo_v[:, columns], preferred_element_type=f32).astype(bf16)
        part[:, :, :, columns] = product.reshape(chips, 2, share, span)
        swap(tile).start()

    def reduce_pairs(tile):
        columns = slice(tile * span, (tile + 1) * span)
        swap(tile).wait()
        for r in range(chips):
            to = lax.rem(chip + r, chips)
            total = part[to, core, :, columns].astype(f32) + pair[to, :, columns].astype(f32)
            if r == 0:
                conv_sum[:, columns] = total
            else:
                both[r, :, columns] = total.astype(bf16)
                exchange(tile, r).start()

    def share_own(q):
        for copy in own_part(q):
            copy.start()

    def share_onward(q):
        for copy, ahead_copy in zip(own_part(q), onward_part(q)):
            copy.wait_recv()
            ahead_copy.start()

    def share_aside(i):
        if i > 0:
            for q in range(2, 4):
                own_part(q)[i - 1].wait_recv()
        aside[i].start()

    jobs = {
        (1, 1): [functools.partial(share_own, 1)],
        (2, 1): [functools.partial(share_own, 2)],
        (3, 1): [functools.partial(share_own, 3)],
        (1, 3): [convolve, functools.partial(filter_rows, 0)],
        (1, 5): [functools.partial(filter_rows, half)],
        (1, 7): [statistics],
        (3, 4): [normalize],
        (4, 1): [functools.partial(share_onward, 0)],
        (5, 1): [functools.partial(share_onward, 1)],
        (6, 0): [functools.partial(share_aside, 0)],
        (7, 0): [functools.partial(share_aside, 1)],
        (8, 0): [functools.partial(share_aside, 2)],
    }
    for tile in range(tiles):
        jobs[4, 3 + tile] = jobs.get((4, 3 + tile), []) + [functools.partial(project, tile)]
        jobs[5, 3 + tile] = jobs.get((5, 3 + tile), []) + [functools.partial(reduce_pairs, tile)]
    last = max(dist + 1, 9)

    @pl.loop(1, last + 1)
    def _(step):
        plus_block = me - step
        minus_block = lax.rem(me + step, n)
        got_plus = (plus_block >= 0) & (step <= dist)
        got_minus = minus_gets(me, step)
        past_plus = plus_block + 1
        past_minus = lax.rem(me + step - 1, n)
        has_plus = (past_plus >= 0) & (step > 1) & (step <= dist + 1)
        has_minus = minus_gets(me, step - 1) & (step > 1) & (me > past_minus)
        plus_arrived = hop(plus_block, step - 1, True)
        plus_onward = hop(plus_block, step, True)
        minus_arrived = hop(minus_block, step - 1, False)
        minus_onward = hop(minus_block, step, False)

        for i in range(9):

            @pl.when(got_plus)
            def _():
                plus_arrived[i].wait_recv()

            @pl.when(got_plus & plus_sends(step))
            def _():
                plus_onward[i].start()

            @pl.when(got_minus)
            def _():
                minus_arrived[i].wait_recv()

            @pl.when(got_minus & minus_sends(step))
            def _():
                minus_onward[i].start()

            if i == 2:

                @pl.when(has_plus)
                def _():
                    for chunk in range(chunks):
                        at, part_sum, lost = attend(past_plus, chunk, None)
                        seen = sum_r[at]
                        acc_r[at] = acc_r[at] + jnp.exp(-seen) * part_sum
                        sum_r[at] = seen + lost

            if i == 6:

                @pl.when(has_minus)
                def _():
                    for chunk in range(chunks):
                        at, part_sum, lost = attend(past_minus, chunk, None)
                        acc_l[at] = part_sum + jnp.exp(-lost) * acc_l[at]
                        sum_l[at] = sum_l[at] + lost

            for at_step, at_piece in jobs:
                if at_piece == i:

                    @pl.when(step == at_step)
                    def _():
                        for job in jobs[at_step, at_piece]:
                            job()

    finish()
    for q in range(2):
        for copy in onward_part(q):
            copy.wait_recv()
    aside[3].start()
    for tile in range(tiles):
        columns = slice(tile * span, (tile + 1) * span)
        total = conv_sum[:, columns]
        for r in range(1, chips):
            exchange(tile, r).wait()
            total = total + recv[r, :, columns].astype(f32)
        conv_sum[:, columns] = total
    for copy in aside:
        copy.wait()
    for q in range(4):
        for copy in own_part(q):
            copy.wait_send()
    for q in range(2):
        for copy in onward_part(q):
            copy.wait_send()
    for r in range(1, tps):
        pass_heads(r).wait()
    all_heads = jnp.concatenate([head_recv[i] for i in range(tps)], axis=1)
    for tile in range(tiles):
        columns = slice(tile * span, (tile + 1) * span)
        product = jnp.dot(all_heads, wa[:, columns], preferred_element_type=f32)
        out_ref[:, columns] = (product + conv_sum[:, columns]).astype(bf16)

    @pl.when(me < n - 1)
    def _():
        halo_copy.wait_send()

    @pl.loop(0, dist)
    def _(step):
        @pl.when(plus_sends(step))
        def _():
            for copy in hop(me - step, step, True):
                copy.wait_send()

        @pl.when(minus_sends(step))
        def _():
            for copy in hop(lax.rem(me + step, n), step, False):
                copy.wait_send()


def local(n, tps, stream, norm_gain, wq, wk, wv, wi, wg, offset, head_gain, taps, cgain, cshift, ao, fo):
    rows, features = stream.shape[1:]
    width = wq.shape[1]
    dist = n // 2
    dma = pltpu.SemaphoreType.DMA
    vmem = pl.BlockSpec(memory_space=pltpu.VMEM)
    anywhere = pl.BlockSpec(memory_space=pltpu.HBM)
    mixed, mass = pl.pallas_call(
        functools.partial(kernel, n, tps),
        out_shape=(
            jax.ShapeDtypeStruct((rows // tps, features), bf16),
            jax.ShapeDtypeStruct((2, rows), f32),
        ),
        in_specs=[anywhere] * 14,
        out_specs=(vmem, vmem),
        scratch_shapes=[
            pltpu.VMEM((rows, features), bf16),
            pltpu.VMEM((features,), bf16),
            pltpu.VMEM((width,), bf16),
            pltpu.VMEM(taps.shape, bf16),
            pltpu.VMEM((width,), bf16),
            pltpu.VMEM((width,), bf16),
            pltpu.VMEM((rows, features), bf16),
            pltpu.VMEM((features, 5 * width), bf16),
            pltpu.VMEM((tps * width, features), bf16),
            pltpu.VMEM((width, features), bf16),
            pltpu.VMEM((n, rows, width), bf16),
            pltpu.VMEM((n, rows, width), bf16),
            pltpu.VMEM((n, 2, rows), bf16),
            pltpu.VMEM((2 * rows, width), bf16),
            pltpu.VMEM((rows, rows), bf16),
            pltpu.VMEM((2 * rows, width), f32),
            pltpu.VMEM((2 * rows, width), f32),
            pltpu.VMEM((2 * rows, width), f32),
            pltpu.VMEM((2 * rows, width), f32),
            pltpu.VMEM((rows, width), bf16),
            pltpu.VMEM((32, width), bf16),
            pltpu.VMEM((rows + 32, width), f32),
            pltpu.VMEM((rows, width), f32),
            pltpu.VMEM((8, rows), f32),
            pltpu.VMEM((tps, 8, rows), f32),
            pltpu.VMEM((rows, width), bf16),
            pltpu.VMEM((tps // 2, 2, rows // tps, features), bf16),
            pltpu.VMEM((tps // 2, rows // tps, features), bf16),
            pltpu.VMEM((tps // 2, rows // tps, features), bf16),
            pltpu.VMEM((tps // 2, rows // tps, features), bf16),
            pltpu.VMEM((rows // tps, features), f32),
            pltpu.VMEM((tps, rows // tps, width), bf16),
            pltpu.VMEM((tps, rows // tps, width), bf16),
            dma((14,)),
            dma((dist, 9)),
            dma((dist, 9)),
            dma((dist, 9)),
            dma((dist, 9)),
            dma((2,)),
            dma((tps,)),
            dma((tps,)),
            dma((2, 4)),
            dma((4, tps // 2)),
            dma((4, tps // 2)),
            dma((16,)),
            dma((16,)),
            dma((tps,)),
            dma((tps,)),
        ],
        compiler_params=pltpu.CompilerParams(
            collective_id=0, has_side_effects=True, vmem_limit_bytes=48000000
        ),
        name="layer",
    )(*[pltpu.with_memory_space_constraint(a, pltpu.HBM) for a in (stream[0], norm_gain, wq, wk, wv, wi, wg, offset[0].T, head_gain, taps, cgain, cshift, ao, fo)])
    return mixed[None], mass.T[None]


def solution(mesh):
    return jax.shard_map(
        functools.partial(local, mesh.shape["sp"], mesh.shape["tp"]),
        mesh=mesh,
        in_specs=(
            P("fs", "sp", None),
            P(),
            P(None, "tp"),
            P(None, "tp"),
            P(None, "tp"),
            P(None, "tp"),
            P(None, "tp"),
            P("fs", "sp", "tp"),
            P("tp"),
            P(None, "tp"),
            P("tp"),
            P("tp"),
            P("tp", None),
            P("tp", None),
        ),
        out_specs=(P("fs", ("sp", "tp"), None), P("fs", "sp", "tp")),
        check_vma=False,
    )
```

```python
import functools

import jax
import jax.numpy as jnp
from jax import lax
from jax.experimental import pallas as pl
from jax.experimental.pallas import tpu as pltpu
from jax.sharding import PartitionSpec as P

HEAD_DIM = 64

rms_eps = 1e-06
norm_eps = 1e-05
mass_floor = 0.01
piece_count = 4
lead = 16

MESH = pl.DeviceIdType.MESH
f32 = jnp.float32
bf16 = jnp.bfloat16


def dot_nt(a, b):
    return lax.dot_general(a, b, (((1,), (1,)), ((), ())), preferred_element_type=f32)


def kernel(
    n,
    tps,
    x_hbm,
    gain_hbm,
    wq_hbm,
    wk_hbm,
    wv_hbm,
    wi_hbm,
    wg_hbm,
    off_hbm,
    head_gain_hbm,
    taps_hbm,
    cgain_hbm,
    cshift_hbm,
    ao_hbm,
    fo_hbm,
    out_ref,
    mass_ref,
    x_v,
    gain_ref,
    head_gain_ref,
    taps_ref,
    cgain_ref,
    cshift_ref,
    normed,
    w_v,
    wa,
    fo_v,
    keep,
    off_v,
    qs,
    tri,
    acc_r,
    sum_r,
    acc_l,
    sum_l,
    gated,
    halo,
    ext,
    filt,
    stat_send,
    stat_recv,
    conv_v,
    part,
    pair,
    both,
    recv,
    conv_sum,
    head_send,
    head_recv,
    load_sem,
    plus_send,
    plus_recv,
    minus_send,
    minus_recv,
    halo_sem,
    pair_sem,
    rs_ssem,
    rs_rsem,
    gather_rsem,
    side_sem,
):
    rows = x_hbm.shape[0]
    width = wq_hbm.shape[1]
    reach = taps_ref.shape[0] - 1
    me = lax.axis_index("sp")
    tp = lax.axis_index("tp")
    right = lax.rem(me + 1, n)
    left = lax.rem(me + n - 1, n)
    dist = n // 2
    low = n - dist - 2

    def rows_of(device):
        return pl.ds(pl.multiple_of(device * width, width), width)

    loads = [
        (x_hbm, x_v),
        (gain_hbm, gain_ref),
        (off_hbm, off_v),
        (wk_hbm, w_v.at[:, 0:width]),
        (wv_hbm, w_v.at[:, width : 2 * width]),
        (wq_hbm, w_v.at[:, 2 * width : 3 * width]),
        (wi_hbm, w_v.at[:, 3 * width : 4 * width]),
        (wg_hbm, w_v.at[:, 4 * width : 5 * width]),
        (ao_hbm, wa.at[rows_of(tp)]),
        (fo_hbm, fo_v),
        (taps_hbm, taps_ref),
        (head_gain_hbm, head_gain_ref),
        (cgain_hbm, cgain_ref),
        (cshift_hbm, cshift_ref),
    ]
    copies = [
        pltpu.make_async_copy(src, dst, load_sem.at[i]) for i, (src, dst) in enumerate(loads)
    ]
    for copy in copies[0:5]:
        copy.start()

    barrier = pltpu.get_barrier_semaphore()
    for neighbour in (left, right):
        pl.semaphore_signal(barrier, inc=1, device_id={"sp": neighbour}, device_id_type=MESH)
    for r in range(1, tps):
        pl.semaphore_signal(
            barrier, inc=1, device_id={"tp": lax.rem(tp + r, tps)}, device_id_type=MESH
        )

    half = rows // 2

    block_rows = lead + 2 * rows
    bounds = [0] + [lead + i * 2 * rows // piece_count for i in range(1, piece_count + 1)]

    def send_piece(slot, step, plus, start, size, i):
        piece = keep.at[slot, pl.ds(start, size)]
        ssem, rsem = (plus_send, plus_recv) if plus else (minus_send, minus_recv)
        return pltpu.make_async_remote_copy(
            src_ref=piece,
            dst_ref=piece,
            send_sem=ssem.at[step],
            recv_sem=rsem.at[step, i],
            device_id={"sp": right if plus else left},
            device_id_type=MESH,
        )

    def hop(slot, step, plus):
        return [
            send_piece(slot, step, plus, bounds[i], bounds[i + 1] - bounds[i], i)
            for i in range(piece_count)
        ]

    def whole(slot, step, plus):
        return send_piece(slot, step, plus, 0, block_rows, 0)

    def plus_sends(step):
        return (me - step >= 0) & (me < n - 1) & (step < dist)

    def minus_gets(device, step):
        block = lax.rem(device + step, n)
        return (step < dist) & (block <= low) & ((device < block) | (device > block + dist))

    def minus_sends(step):
        block = lax.rem(me + step, n)
        fits = (step == 0) | minus_gets(me, step)
        return fits & (block <= low) & minus_gets(left, step + 1)

    row_id = lax.broadcasted_iota(jnp.int32, (rows, rows), 0)
    col_id = lax.broadcasted_iota(jnp.int32, (rows, rows), 1)
    tri[...] = (row_id > col_id).astype(f32).astype(bf16)

    copies[1].wait()
    gain = gain_ref[...].astype(f32).reshape(1, gain_ref.shape[0])
    copies[0].wait()
    for copy in copies[5:]:
        copy.start()

    @pl.loop(0, rows // 32)
    def _(i):
        at = pl.ds(pl.multiple_of(i * 32, 32), 32)
        xf = x_v[at].astype(f32)
        scale = lax.rsqrt(jnp.mean(xf * xf, axis=-1, keepdims=True) + rms_eps)
        normed[at] = (xf * scale * gain).astype(bf16)

    for i in (2, 3, 4):
        copies[i].wait()
    kv = jnp.dot(normed[...], w_v[:, 0 : 2 * width], preferred_element_type=f32)
    keep[me, lead : lead + rows] = kv[:, 0:width].astype(bf16)
    keep[me, lead + rows : block_rows] = kv[:, width : 2 * width].astype(bf16)
    offsets = off_v[...].astype(f32)
    lines = [offsets[h : h + 1, i : i + width] for h in range(2) for i in range(0, rows, width)]
    lines.append(jnp.zeros((lead - len(lines), width), f32))
    keep[me, 0:lead] = jnp.concatenate(lines, axis=0).astype(bf16)

    pl.semaphore_wait(barrier, tps + 1)

    @pl.when(plus_sends(0))
    def _():
        for copy in hop(me, 0, True):
            copy.start()

    @pl.when(minus_sends(0))
    def _():
        for copy in hop(me, 0, False):
            copy.start()

    chips = tps // 2
    chip, core = tp // 2, lax.rem(tp, 2)
    sibling = tp + 1 - 2 * core
    ahead = 2 * lax.rem(chip + 1, chips) + core
    behind = 2 * lax.rem(chip + chips - 1, chips) + core
    across = 2 * lax.rem(chip + 2, chips) + core
    fold = width // 4

    def spread(i, device, to, start=0, size=width):
        part_rows = wa.at[pl.ds(pl.multiple_of(device * width + start, fold), size)]
        return pltpu.make_async_remote_copy(
            src_ref=part_rows,
            dst_ref=part_rows,
            send_sem=side_sem.at[4],
            recv_sem=gather_rsem.at[i],
            device_id={"tp": to},
            device_id_type=MESH,
        )

    def own_part(q):
        return (
            spread(q, tp, ahead, q * fold, fold),
            spread(4 + q, tp, behind, lax.rem(q + 2, 4) * fold, fold),
        )

    def onward_part(q):
        return (
            spread(8 + q, behind, ahead, q * fold, fold),
            spread(10 + q, ahead, behind, (q + 2) * fold, fold),
        )

    aside = [spread(12 + i, device, sibling) for i, device in enumerate((tp, behind, ahead, across))]
    copies[8].wait()
    for copy in own_part(0):
        copy.start()

    for i in (5, 6, 7):
        copies[i].wait()
    qig = jnp.dot(normed[...], w_v[:, 2 * width : 5 * width], preferred_element_type=f32)
    gate = qig[:, 2 * width : 3 * width].astype(bf16).astype(f32)
    conv_in = qig[:, width : 2 * width].astype(bf16).astype(f32)
    gated_rows = (conv_in * (1.0 / (1.0 + jnp.exp(-gate)))).astype(bf16)
    gated[...] = gated_rows
    tail = 32
    halo_copy = pltpu.make_async_remote_copy(
        src_ref=gated.at[pl.ds(rows - tail, tail)],
        dst_ref=halo,
        send_sem=halo_sem.at[0],
        recv_sem=halo_sem.at[1],
        device_id={"sp": right},
        device_id_type=MESH,
    )

    @pl.when(me < n - 1)
    def _():
        halo_copy.start()

    lane = lax.broadcasted_iota(jnp.int32, (rows, width), 1)
    first = lane < HEAD_DIM
    query = qig[:, 0:width].astype(bf16).astype(f32) * HEAD_DIM ** (-0.5)
    qs[0:rows] = jnp.where(first, query, 0.0).astype(bf16)
    qs[rows : 2 * rows] = jnp.where(first, 0.0, query).astype(bf16)

    def attend(slot, chunk, strict):
        head = chunk * half // rows
        at = pl.ds(chunk * half, half)
        lines = keep[slot, 0:lead].astype(f32)
        per_head = rows // width
        offset = jnp.concatenate(
            [lines[i : i + 1] for i in range(head * per_head, (head + 1) * per_head)], axis=1
        )
        scores = dot_nt(qs[at], keep[slot, lead : lead + rows]) + offset
        soft = jnp.maximum(jnp.log(1.0 + jnp.exp(jnp.minimum(scores, 80.0))), scores)
        gain_log = scores - soft
        if strict is not None:
            soft = jnp.where(strict, soft, 0.0)
        beyond = jnp.dot(soft.astype(bf16), tri[...], preferred_element_type=f32)
        weights = jnp.exp(gain_log - beyond)
        if strict is not None:
            weights = jnp.where(strict, weights, 0.0)
        part_sum = jnp.dot(weights.astype(bf16), keep[slot, lead + rows : block_rows], preferred_element_type=f32)
        lost = jnp.broadcast_to(beyond[:, 0:1] + soft[:, 0:1], (half, width))
        return at, part_sum, lost

    chunks = 2 * rows // half
    for chunk in range(chunks):
        base = chunk * half % rows
        query_pos = lax.broadcasted_iota(jnp.int32, (half, rows), 0) + base
        key_pos = lax.broadcasted_iota(jnp.int32, (half, rows), 1)
        at, part_sum, lost = attend(me, chunk, key_pos < query_pos)
        acc_r[at] = part_sum
        sum_r[at] = lost
    for i in (10, 11, 12, 13):
        copies[i].wait()
    acc_l[...] = jnp.zeros_like(acc_l)
    sum_l[...] = jnp.zeros_like(sum_l)

    stat_copies = [
        pltpu.make_async_remote_copy(
            src_ref=stat_send,
            dst_ref=stat_recv.at[r],
            send_sem=side_sem.at[0],
            recv_sem=side_sem.at[1],
            device_id={"tp": lax.rem(tp + r, tps)},
            device_id_type=MESH,
        )
        for r in range(1, tps)
    ]

    def convolve():
        @pl.when(me > 0)
        def _():
            halo_copy.wait_recv()
            ext[0:tail] = halo[...].astype(f32)

        @pl.when(me == 0)
        def _():
            ext[0:tail] = jnp.zeros((tail, width), f32)

        ext[tail : tail + rows] = gated[...].astype(f32)

    def filter_rows(base):
        taps = taps_ref[...].astype(f32)
        total = jnp.zeros((half, width), f32)
        for k in range(reach + 1):
            total = total + ext[base + tail - reach + k : base + tail - reach + k + half] * taps[k : k + 1]
        filt[base : base + half] = total

    def statistics():
        filtered = filt[...]
        sums = jnp.sum(filtered, axis=-1, keepdims=True)
        squares = jnp.sum(filtered * filtered, axis=-1, keepdims=True)
        packed = jnp.where(lane == 0, sums, squares)
        stat_send[...] = packed.T[0:8]
        for copy in stat_copies:
            copy.start()

    def normalize():
        total = stat_send[...]
        pltpu.make_async_remote_copy(
            src_ref=stat_recv.at[pl.ds(1, tps - 1)],
            dst_ref=stat_recv.at[pl.ds(1, tps - 1)],
            send_sem=side_sem.at[0],
            recv_sem=side_sem.at[1],
            device_id={"tp": sibling},
            device_id_type=MESH,
        ).wait()
        for r in range(1, tps):
            total = total + stat_recv[r]
        mean = total / (width * tps)
        center = mean[0:1]
        spread = jnp.maximum(mean[1:2] - center * center, 0.0)
        scale = lax.rsqrt(spread + norm_eps)
        line = lax.broadcasted_iota(jnp.int32, (width, rows), 0)
        columns = jnp.where(line == 0, center, scale).T
        hidden = (filt[...] - columns[:, 0:1]) * columns[:, 1:2]
        hidden = hidden * cgain_ref[...].astype(f32).reshape(1, width)
        hidden = hidden + cshift_ref[...].astype(f32).reshape(1, width)
        conv_v[...] = (hidden * (1.0 / (1.0 + jnp.exp(-hidden)))).astype(bf16)
        copies[9].wait()

    features = wa.shape[1]
    share = rows // tps
    tiles = 4
    span = features // tiles

    def swap(tile):
        columns = pl.ds(tile * span, span)
        return pltpu.make_async_remote_copy(
            src_ref=part.at[:, 1 - core, :, columns],
            dst_ref=pair.at[:, :, columns],
            send_sem=pair_sem.at[0, tile],
            recv_sem=pair_sem.at[1, tile],
            device_id={"tp": sibling},
            device_id_type=MESH,
        )

    def exchange(tile, r):
        columns = pl.ds(tile * span, span)
        return pltpu.make_async_remote_copy(
            src_ref=both.at[r, :, columns],
            dst_ref=recv.at[r, :, columns],
            send_sem=rs_ssem.at[tile],
            recv_sem=rs_rsem.at[tile],
            device_id={"tp": 2 * lax.rem(chip + r, chips) + core},
            device_id_type=MESH,
        )

    def finish():
        attended = acc_r[...] + jnp.exp(-sum_r[...]) * acc_l[...]
        lost = sum_r[...] + sum_l[...]
        mass = jnp.log(jnp.maximum(1.0 - jnp.exp(-jnp.where(first, lost[0:rows], lost[rows : 2 * rows])), mass_floor)).T
        mass_ref[0:1] = mass[0:1]
        mass_ref[1:2] = mass[HEAD_DIM : HEAD_DIM + 1]
        attended = jnp.where(first, attended[0:rows], attended[rows : 2 * rows])
        power = attended * attended
        low_mean = jnp.sum(jnp.where(first, power, 0.0), axis=-1, keepdims=True) / HEAD_DIM
        high_mean = jnp.sum(jnp.where(first, 0.0, power), axis=-1, keepdims=True) / HEAD_DIM
        scale = jnp.where(first, lax.rsqrt(low_mean + rms_eps), lax.rsqrt(high_mean + rms_eps))
        heads = attended * scale * head_gain_ref[...].astype(f32).reshape(1, width)
        head_send[...] = heads.astype(bf16).reshape(tps, share, width)
        for r in range(1, tps):
            pass_heads(r).start()
        head_recv[tp] = head_send[tp]

    def pass_heads(r):
        peer = lax.rem(tp + r, tps)
        return pltpu.make_async_remote_copy(
            src_ref=head_send.at[peer],
            dst_ref=head_recv.at[tp],
            send_sem=side_sem.at[2],
            recv_sem=side_sem.at[3],
            device_id={"tp": peer},
            device_id_type=MESH,
        )

    def project(tile):
        columns = slice(tile * span, (tile + 1) * span)
        product = jnp.dot(conv_v[...], fo_v[:, columns], preferred_element_type=f32).astype(bf16)
        part[:, :, :, columns] = product.reshape(chips, 2, share, span)
        swap(tile).start()

    def reduce_pairs(tile):
        columns = slice(tile * span, (tile + 1) * span)
        swap(tile).wait()
        for r in range(chips):
            to = lax.rem(chip + r, chips)
            total = part[to, core, :, columns].astype(f32) + pair[to, :, columns].astype(f32)
            if r == 0:
                conv_sum[:, columns] = total
            else:
                both[r, :, columns] = total.astype(bf16)
                exchange(tile, r).start()

    def share_own(q):
        for copy in own_part(q):
            copy.start()

    def share_onward(q):
        for copy, ahead_copy in zip(own_part(q), onward_part(q)):
            copy.wait_recv()
            ahead_copy.start()

    def share_aside(i):
        if i > 0:
            for q in range(2, 4):
                own_part(q)[i - 1].wait_recv()
        aside[i].start()

    jobs = {
        (1, 1): [functools.partial(share_own, 1)],
        (2, 1): [functools.partial(share_own, 2)],
        (3, 1): [functools.partial(share_own, 3)],
        (1, 3): [convolve, functools.partial(filter_rows, 0)],
        (1, 5): [functools.partial(filter_rows, half)],
        (1, 7): [statistics],
        (3, 4): [normalize],
        (4, 1): [functools.partial(share_onward, 0)],
        (5, 1): [functools.partial(share_onward, 1)],
        (6, 0): [functools.partial(share_aside, 0)],
        (7, 0): [functools.partial(share_aside, 1)],
        (8, 0): [functools.partial(share_aside, 2)],
    }
    for tile in range(tiles):
        jobs[4, 3 + tile] = jobs.get((4, 3 + tile), []) + [functools.partial(project, tile)]
        jobs[5, 3 + tile] = jobs.get((5, 3 + tile), []) + [functools.partial(reduce_pairs, tile)]
    last = max(dist + 1, 9)

    @pl.loop(1, last + 1)
    def _(step):
        plus_block = me - step
        minus_block = lax.rem(me + step, n)
        got_plus = (plus_block >= 0) & (step <= dist)
        got_minus = minus_gets(me, step)
        past_plus = plus_block + 1
        past_minus = lax.rem(me + step - 1, n)
        has_plus = (past_plus >= 0) & (step > 1) & (step <= dist + 1)
        has_minus = minus_gets(me, step - 1) & (step > 1) & (me > past_minus)
        plus_arrived = hop(plus_block, step - 1, True)
        plus_onward = hop(plus_block, step, True)
        minus_arrived = hop(minus_block, step - 1, False)
        minus_onward = hop(minus_block, step, False)

        for i in range(8):
            piece, rest = divmod(i * piece_count, 8)

            if rest == 0:

                @pl.when(got_plus)
                def _():
                    plus_arrived[piece].wait_recv()

                @pl.when(got_plus & plus_sends(step))
                def _():
                    plus_onward[piece].start()

                @pl.when(got_minus)
                def _():
                    minus_arrived[piece].wait_recv()

                @pl.when(got_minus & minus_sends(step))
                def _():
                    minus_onward[piece].start()

            if i == 2:

                @pl.when(has_plus)
                def _():
                    for chunk in range(chunks):
                        at, part_sum, lost = attend(past_plus, chunk, None)
                        seen = sum_r[at]
                        acc_r[at] = acc_r[at] + jnp.exp(-seen) * part_sum
                        sum_r[at] = seen + lost

            if i == 6:

                @pl.when(has_minus)
                def _():
                    for chunk in range(chunks):
                        at, part_sum, lost = attend(past_minus, chunk, None)
                        acc_l[at] = part_sum + jnp.exp(-lost) * acc_l[at]
                        sum_l[at] = sum_l[at] + lost

            for at_step, at_piece in jobs:
                if at_piece == i:

                    @pl.when(step == at_step)
                    def _():
                        for job in jobs[at_step, at_piece]:
                            job()

    finish()
    for q in range(2):
        for copy in onward_part(q):
            copy.wait_recv()
    aside[3].start()
    for tile in range(tiles):
        columns = slice(tile * span, (tile + 1) * span)
        total = conv_sum[:, columns]
        pltpu.make_async_remote_copy(
            src_ref=both.at[pl.ds(1, chips - 1), :, columns],
            dst_ref=recv.at[pl.ds(1, chips - 1), :, columns],
            send_sem=rs_ssem.at[tile],
            recv_sem=rs_rsem.at[tile],
            device_id={"tp": sibling},
            device_id_type=MESH,
        ).wait()
        for r in range(1, chips):
            total = total + recv[r, :, columns].astype(f32)
        conv_sum[:, columns] = total
    for copy in aside:
        copy.wait_recv()
    spread(12, 0, sibling, 0, 4 * width + 12 * fold).wait_send()
    pltpu.make_async_remote_copy(
        src_ref=head_send.at[pl.ds(1, tps - 1)],
        dst_ref=head_recv.at[pl.ds(1, tps - 1)],
        send_sem=side_sem.at[2],
        recv_sem=side_sem.at[3],
        device_id={"tp": sibling},
        device_id_type=MESH,
    ).wait()
    all_heads = jnp.concatenate([head_recv[i] for i in range(tps)], axis=1)
    for tile in range(tiles):
        columns = slice(tile * span, (tile + 1) * span)
        product = jnp.dot(all_heads, wa[:, columns], preferred_element_type=f32)
        out_ref[:, columns] = (product + conv_sum[:, columns]).astype(bf16)

    @pl.when(me < n - 1)
    def _():
        halo_copy.wait_send()

    @pl.loop(0, dist)
    def _(step):
        @pl.when(plus_sends(step))
        def _():
            whole(me - step, step, True).wait_send()

        @pl.when(minus_sends(step))
        def _():
            whole(lax.rem(me + step, n), step, False).wait_send()


def local(n, tps, stream, norm_gain, wq, wk, wv, wi, wg, offset, head_gain, taps, cgain, cshift, ao, fo):
    rows, features = stream.shape[1:]
    width = wq.shape[1]
    dist = n // 2
    dma = pltpu.SemaphoreType.DMA
    vmem = pl.BlockSpec(memory_space=pltpu.VMEM)
    anywhere = pl.BlockSpec(memory_space=pltpu.HBM)
    mixed, mass = pl.pallas_call(
        functools.partial(kernel, n, tps),
        out_shape=(
            jax.ShapeDtypeStruct((rows // tps, features), bf16),
            jax.ShapeDtypeStruct((2, rows), f32),
        ),
        in_specs=[anywhere] * 14,
        out_specs=(vmem, vmem),
        scratch_shapes=[
            pltpu.VMEM((rows, features), bf16),
            pltpu.VMEM((features,), bf16),
            pltpu.VMEM((width,), bf16),
            pltpu.VMEM(taps.shape, bf16),
            pltpu.VMEM((width,), bf16),
            pltpu.VMEM((width,), bf16),
            pltpu.VMEM((rows, features), bf16),
            pltpu.VMEM((features, 5 * width), bf16),
            pltpu.VMEM((tps * width, features), bf16),
            pltpu.VMEM((width, features), bf16),
            pltpu.VMEM((n, lead + 2 * rows, width), bf16),
            pltpu.VMEM((2, rows), bf16),
            pltpu.VMEM((2 * rows, width), bf16),
            pltpu.VMEM((rows, rows), bf16),
            pltpu.VMEM((2 * rows, width), f32),
            pltpu.VMEM((2 * rows, width), f32),
            pltpu.VMEM((2 * rows, width), f32),
            pltpu.VMEM((2 * rows, width), f32),
            pltpu.VMEM((rows, width), bf16),
            pltpu.VMEM((32, width), bf16),
            pltpu.VMEM((rows + 32, width), f32),
            pltpu.VMEM((rows, width), f32),
            pltpu.VMEM((8, rows), f32),
            pltpu.VMEM((tps, 8, rows), f32),
            pltpu.VMEM((rows, width), bf16),
            pltpu.VMEM((tps // 2, 2, rows // tps, features), bf16),
            pltpu.VMEM((tps // 2, rows // tps, features), bf16),
            pltpu.VMEM((tps // 2, rows // tps, features), bf16),
            pltpu.VMEM((tps // 2, rows // tps, features), bf16),
            pltpu.VMEM((rows // tps, features), f32),
            pltpu.VMEM((tps, rows // tps, width), bf16),
            pltpu.VMEM((tps, rows // tps, width), bf16),
            dma((14,)),
            dma((dist,)),
            dma((dist, piece_count)),
            dma((dist,)),
            dma((dist, piece_count)),
            dma((2,)),
            dma((2, 4)),
            dma((4,)),
            dma((4,)),
            dma((16,)),
            dma((5,)),
        ],
        compiler_params=pltpu.CompilerParams(
            collective_id=0, has_side_effects=True, vmem_limit_bytes=48000000
        ),
        name="layer",
    )(*[pltpu.with_memory_space_constraint(a, pltpu.HBM) for a in (stream[0], norm_gain, wq, wk, wv, wi, wg, offset[0].T, head_gain, taps, cgain, cshift, ao, fo)])
    return mixed[None], mass.T[None]


def solution(mesh):
    return jax.shard_map(
        functools.partial(local, mesh.shape["sp"], mesh.shape["tp"]),
        mesh=mesh,
        in_specs=(
            P("fs", "sp", None),
            P(),
            P(None, "tp"),
            P(None, "tp"),
            P(None, "tp"),
            P(None, "tp"),
            P(None, "tp"),
            P("fs", "sp", "tp"),
            P("tp"),
            P(None, "tp"),
            P("tp"),
            P("tp"),
            P("tp", None),
            P("tp", None),
        ),
        out_specs=(P("fs", ("sp", "tp"), None), P("fs", "sp", "tp")),
        check_vma=False,
    )
```

```python
import functools

import jax
import jax.numpy as jnp
from jax import lax
from jax.experimental import pallas as pl
from jax.experimental.pallas import tpu as pltpu
from jax.sharding import PartitionSpec as P

HEAD_DIM = 64

rms_eps = 1e-06
norm_eps = 1e-05
mass_floor = 0.01
piece_count = 4
lead = 16

MESH = pl.DeviceIdType.MESH
f32 = jnp.float32
bf16 = jnp.bfloat16


def dot_nt(a, b):
    return lax.dot_general(a, b, (((1,), (1,)), ((), ())), preferred_element_type=f32)


def kernel(
    n,
    tps,
    x_hbm,
    gain_hbm,
    wq_hbm,
    wk_hbm,
    wv_hbm,
    wi_hbm,
    wg_hbm,
    off_hbm,
    head_gain_hbm,
    taps_hbm,
    cgain_hbm,
    cshift_hbm,
    ao_hbm,
    fo_hbm,
    out_ref,
    mass_ref,
    x_v,
    gain_ref,
    head_gain_ref,
    taps_ref,
    cgain_ref,
    cshift_ref,
    normed,
    w_v,
    wa,
    fo_v,
    keep,
    off_v,
    qs,
    tri,
    acc_r,
    sum_r,
    acc_l,
    sum_l,
    gated,
    halo,
    ext,
    filt,
    stat_send,
    stat_recv,
    conv_v,
    part,
    pair,
    both,
    recv,
    conv_sum,
    head_send,
    head_recv,
    load_sem,
    plus_send,
    plus_recv,
    minus_send,
    minus_recv,
    halo_sem,
    pair_sem,
    rs_ssem,
    rs_rsem,
    gather_rsem,
    side_sem,
):
    rows = x_hbm.shape[0]
    width = wq_hbm.shape[1]
    reach = taps_ref.shape[0] - 1
    me = lax.axis_index("sp")
    tp = lax.axis_index("tp")
    right = lax.rem(me + 1, n)
    left = lax.rem(me + n - 1, n)
    dist = n // 2
    low = n - dist - 2

    def rows_of(device):
        return pl.ds(pl.multiple_of(device * width, width), width)

    loads = [
        (x_hbm, x_v),
        (gain_hbm, gain_ref),
        (off_hbm, off_v),
        (wk_hbm, w_v.at[:, 0:width]),
        (wv_hbm, w_v.at[:, width : 2 * width]),
        (wq_hbm, w_v.at[:, 2 * width : 3 * width]),
        (wi_hbm, w_v.at[:, 3 * width : 4 * width]),
        (wg_hbm, w_v.at[:, 4 * width : 5 * width]),
        (ao_hbm, wa.at[rows_of(tp)]),
        (fo_hbm, fo_v),
        (taps_hbm, taps_ref),
        (head_gain_hbm, head_gain_ref),
        (cgain_hbm, cgain_ref),
        (cshift_hbm, cshift_ref),
    ]
    copies = [
        pltpu.make_async_copy(src, dst, load_sem.at[i]) for i, (src, dst) in enumerate(loads)
    ]
    for copy in copies[0:5]:
        copy.start()

    barrier = pltpu.get_barrier_semaphore()
    for neighbour in (left, right):
        pl.semaphore_signal(barrier, inc=1, device_id={"sp": neighbour}, device_id_type=MESH)
    for r in range(1, tps):
        pl.semaphore_signal(
            barrier, inc=1, device_id={"tp": lax.rem(tp + r, tps)}, device_id_type=MESH
        )

    half = rows // 2

    block_rows = lead + 2 * rows
    bounds = [0] + [lead + i * 2 * rows // piece_count for i in range(1, piece_count + 1)]

    def send_piece(slot, step, plus, start, size, i):
        piece = keep.at[slot, pl.ds(start, size)]
        ssem, rsem = (plus_send, plus_recv) if plus else (minus_send, minus_recv)
        return pltpu.make_async_remote_copy(
            src_ref=piece,
            dst_ref=piece,
            send_sem=ssem.at[step],
            recv_sem=rsem.at[step, i],
            device_id={"sp": right if plus else left},
            device_id_type=MESH,
        )

    def hop(slot, step, plus):
        return [
            send_piece(slot, step, plus, bounds[i], bounds[i + 1] - bounds[i], i)
            for i in range(piece_count)
        ]

    def whole(slot, step, plus):
        return send_piece(slot, step, plus, 0, block_rows, 0)

    def plus_sends(step):
        return (me - step >= 0) & (me < n - 1) & (step < dist)

    def minus_gets(device, step):
        block = lax.rem(device + step, n)
        return (step < dist) & (block <= low) & ((device < block) | (device > block + dist))

    def minus_sends(step):
        block = lax.rem(me + step, n)
        fits = (step == 0) | minus_gets(me, step)
        return fits & (block <= low) & minus_gets(left, step + 1)

    row_id = lax.broadcasted_iota(jnp.int32, (rows, rows), 0)
    col_id = lax.broadcasted_iota(jnp.int32, (rows, rows), 1)
    tri[...] = (row_id > col_id).astype(f32).astype(bf16)

    copies[1].wait()
    gain = gain_ref[...].astype(f32).reshape(1, gain_ref.shape[0])
    copies[0].wait()
    for copy in copies[5:]:
        copy.start()

    @pl.loop(0, rows // 32)
    def _(i):
        at = pl.ds(pl.multiple_of(i * 32, 32), 32)
        xf = x_v[at].astype(f32)
        scale = lax.rsqrt(jnp.mean(xf * xf, axis=-1, keepdims=True) + rms_eps)
        normed[at] = (xf * scale * gain).astype(bf16)

    for i in (2, 3, 4):
        copies[i].wait()
    kv = jnp.dot(normed[...], w_v[:, 0 : 2 * width], preferred_element_type=f32)
    keep[me, lead : lead + rows] = kv[:, 0:width].astype(bf16)
    keep[me, lead + rows : block_rows] = kv[:, width : 2 * width].astype(bf16)
    offsets = off_v[...].astype(f32)
    lines = [offsets[h : h + 1, i : i + width] for h in range(2) for i in range(0, rows, width)]
    lines.append(jnp.zeros((lead - len(lines), width), f32))
    keep[me, 0:lead] = jnp.concatenate(lines, axis=0).astype(bf16)

    pl.semaphore_wait(barrier, tps + 1)

    @pl.when(plus_sends(0))
    def _():
        for copy in hop(me, 0, True):
            copy.start()

    @pl.when(minus_sends(0))
    def _():
        for copy in hop(me, 0, False):
            copy.start()

    chips = tps // 2
    chip, core = tp // 2, lax.rem(tp, 2)
    sibling = tp + 1 - 2 * core
    ahead = 2 * lax.rem(chip + 1, chips) + core
    behind = 2 * lax.rem(chip + chips - 1, chips) + core
    across = 2 * lax.rem(chip + 2, chips) + core
    fold = width // 4

    def spread(i, device, to, start=0, size=width):
        part_rows = wa.at[pl.ds(pl.multiple_of(device * width + start, fold), size)]
        return pltpu.make_async_remote_copy(
            src_ref=part_rows,
            dst_ref=part_rows,
            send_sem=side_sem.at[4],
            recv_sem=gather_rsem.at[i],
            device_id={"tp": to},
            device_id_type=MESH,
        )

    def own_part(q):
        return (
            spread(q, tp, ahead, q * fold, fold),
            spread(4 + q, tp, behind, lax.rem(q + 2, 4) * fold, fold),
        )

    def onward_part(q):
        return (
            spread(8 + q, behind, ahead, q * fold, fold),
            spread(10 + q, ahead, behind, (q + 2) * fold, fold),
        )

    aside = [spread(12 + i, device, sibling) for i, device in enumerate((tp, behind, ahead, across))]
    copies[8].wait()
    for copy in own_part(0):
        copy.start()

    for i in (5, 6, 7):
        copies[i].wait()
    qig = jnp.dot(normed[...], w_v[:, 2 * width : 5 * width], preferred_element_type=f32)
    gate = qig[:, 2 * width : 3 * width].astype(bf16).astype(f32)
    conv_in = qig[:, width : 2 * width].astype(bf16).astype(f32)
    gated_rows = (conv_in * (1.0 / (1.0 + jnp.exp(-gate)))).astype(bf16)
    gated[...] = gated_rows
    tail = 32
    halo_copy = pltpu.make_async_remote_copy(
        src_ref=gated.at[pl.ds(rows - tail, tail)],
        dst_ref=halo,
        send_sem=halo_sem.at[0],
        recv_sem=halo_sem.at[1],
        device_id={"sp": right},
        device_id_type=MESH,
    )

    @pl.when(me < n - 1)
    def _():
        halo_copy.start()

    lane = lax.broadcasted_iota(jnp.int32, (rows, width), 1)
    first = lane < HEAD_DIM
    query = qig[:, 0:width].astype(bf16).astype(f32) * HEAD_DIM ** (-0.5)
    qs[0:rows] = jnp.where(first, query, 0.0).astype(bf16)
    qs[rows : 2 * rows] = jnp.where(first, 0.0, query).astype(bf16)

    def attend(slot, chunk, strict):
        at = pl.ds(0, 2 * rows)
        lines = keep[slot, 0:lead].astype(f32)
        per_head = rows // width
        offset = jnp.concatenate(
            [
                jnp.broadcast_to(
                    jnp.concatenate(
                        [lines[head * per_head + i : head * per_head + i + 1] for i in range(per_head)],
                        axis=1,
                    ),
                    (rows, rows),
                )
                for head in range(2)
            ],
            axis=0,
        )
        scores = dot_nt(qs[at], keep[slot, lead : lead + rows]) + offset
        soft = jnp.maximum(jnp.log(1.0 + jnp.exp(jnp.minimum(scores, 80.0))), scores)
        gain_log = scores - soft
        if strict is not None:
            soft = jnp.where(strict, soft, 0.0)
        beyond = jnp.dot(soft.astype(bf16), tri[...], preferred_element_type=f32)
        weights = jnp.exp(gain_log - beyond)
        if strict is not None:
            weights = jnp.where(strict, weights, 0.0)
        part_sum = jnp.dot(weights.astype(bf16), keep[slot, lead + rows : block_rows], preferred_element_type=f32)
        lost = jnp.broadcast_to(beyond[:, 0:1] + soft[:, 0:1], (2 * rows, width))
        return at, part_sum, lost

    chunks = 1
    for chunk in range(chunks):
        at, part_sum, lost = attend(me, chunk, jnp.concatenate([col_id < row_id] * 2, axis=0))
        acc_r[at] = part_sum
        sum_r[at] = lost
    for i in (10, 11, 12, 13):
        copies[i].wait()
    acc_l[...] = jnp.zeros_like(acc_l)
    sum_l[...] = jnp.zeros_like(sum_l)

    stat_copies = [
        pltpu.make_async_remote_copy(
            src_ref=stat_send,
            dst_ref=stat_recv.at[r],
            send_sem=side_sem.at[0],
            recv_sem=side_sem.at[1],
            device_id={"tp": lax.rem(tp + r, tps)},
            device_id_type=MESH,
        )
        for r in range(1, tps)
    ]

    def convolve():
        @pl.when(me > 0)
        def _():
            halo_copy.wait_recv()
            ext[0:tail] = halo[...].astype(f32)

        @pl.when(me == 0)
        def _():
            ext[0:tail] = jnp.zeros((tail, width), f32)

        ext[tail : tail + rows] = gated[...].astype(f32)

    def filter_rows(base):
        taps = taps_ref[...].astype(f32)
        total = jnp.zeros((half, width), f32)
        for k in range(reach + 1):
            total = total + ext[base + tail - reach + k : base + tail - reach + k + half] * taps[k : k + 1]
        filt[base : base + half] = total

    def statistics():
        filtered = filt[...]
        sums = jnp.sum(filtered, axis=-1, keepdims=True)
        squares = jnp.sum(filtered * filtered, axis=-1, keepdims=True)
        packed = jnp.where(lane == 0, sums, squares)
        stat_send[...] = packed.T[0:8]
        for copy in stat_copies:
            copy.start()

    def normalize():
        total = stat_send[...]
        pltpu.make_async_remote_copy(
            src_ref=stat_recv.at[pl.ds(1, tps - 1)],
            dst_ref=stat_recv.at[pl.ds(1, tps - 1)],
            send_sem=side_sem.at[0],
            recv_sem=side_sem.at[1],
            device_id={"tp": sibling},
            device_id_type=MESH,
        ).wait()
        for r in range(1, tps):
            total = total + stat_recv[r]
        mean = total / (width * tps)
        center = mean[0:1]
        spread = jnp.maximum(mean[1:2] - center * center, 0.0)
        scale = lax.rsqrt(spread + norm_eps)
        line = lax.broadcasted_iota(jnp.int32, (width, rows), 0)
        columns = jnp.where(line == 0, center, scale).T
        hidden = (filt[...] - columns[:, 0:1]) * columns[:, 1:2]
        hidden = hidden * cgain_ref[...].astype(f32).reshape(1, width)
        hidden = hidden + cshift_ref[...].astype(f32).reshape(1, width)
        conv_v[...] = (hidden * (1.0 / (1.0 + jnp.exp(-hidden)))).astype(bf16)
        copies[9].wait()

    features = wa.shape[1]
    share = rows // tps
    tiles = 4
    span = features // tiles

    def swap(tile):
        columns = pl.ds(tile * span, span)
        return pltpu.make_async_remote_copy(
            src_ref=part.at[:, 1 - core, :, columns],
            dst_ref=pair.at[:, :, columns],
            send_sem=pair_sem.at[0, tile],
            recv_sem=pair_sem.at[1, tile],
            device_id={"tp": sibling},
            device_id_type=MESH,
        )

    def exchange(tile, r):
        columns = pl.ds(tile * span, span)
        return pltpu.make_async_remote_copy(
            src_ref=both.at[r, :, columns],
            dst_ref=recv.at[r, :, columns],
            send_sem=rs_ssem.at[tile],
            recv_sem=rs_rsem.at[tile],
            device_id={"tp": 2 * lax.rem(chip + r, chips) + core},
            device_id_type=MESH,
        )

    def finish():
        attended = acc_r[...] + jnp.exp(-sum_r[...]) * acc_l[...]
        lost = sum_r[...] + sum_l[...]
        mass = jnp.log(jnp.maximum(1.0 - jnp.exp(-jnp.where(first, lost[0:rows], lost[rows : 2 * rows])), mass_floor)).T
        mass_ref[0:1] = mass[0:1]
        mass_ref[1:2] = mass[HEAD_DIM : HEAD_DIM + 1]
        attended = jnp.where(first, attended[0:rows], attended[rows : 2 * rows])
        power = attended * attended
        low_mean = jnp.sum(jnp.where(first, power, 0.0), axis=-1, keepdims=True) / HEAD_DIM
        high_mean = jnp.sum(jnp.where(first, 0.0, power), axis=-1, keepdims=True) / HEAD_DIM
        scale = jnp.where(first, lax.rsqrt(low_mean + rms_eps), lax.rsqrt(high_mean + rms_eps))
        heads = attended * scale * head_gain_ref[...].astype(f32).reshape(1, width)
        head_send[...] = heads.astype(bf16).reshape(tps, share, width)
        for r in range(1, tps):
            pass_heads(r).start()
        head_recv[tp] = head_send[tp]

    def pass_heads(r):
        peer = lax.rem(tp + r, tps)
        return pltpu.make_async_remote_copy(
            src_ref=head_send.at[peer],
            dst_ref=head_recv.at[tp],
            send_sem=side_sem.at[2],
            recv_sem=side_sem.at[3],
            device_id={"tp": peer},
            device_id_type=MESH,
        )

    def project(tile):
        columns = slice(tile * span, (tile + 1) * span)
        product = jnp.dot(conv_v[...], fo_v[:, columns], preferred_element_type=f32).astype(bf16)
        part[:, :, :, columns] = product.reshape(chips, 2, share, span)
        swap(tile).start()

    def reduce_pairs(tile):
        columns = slice(tile * span, (tile + 1) * span)
        swap(tile).wait()
        for r in range(chips):
            to = lax.rem(chip + r, chips)
            total = part[to, core, :, columns].astype(f32) + pair[to, :, columns].astype(f32)
            if r == 0:
                conv_sum[:, columns] = total
            else:
                both[r, :, columns] = total.astype(bf16)
                exchange(tile, r).start()

    def share_own(q):
        for copy in own_part(q):
            copy.start()

    def share_onward(q):
        for copy, ahead_copy in zip(own_part(q), onward_part(q)):
            copy.wait_recv()
            ahead_copy.start()

    def share_aside(i):
        if i > 0:
            for q in range(2, 4):
                own_part(q)[i - 1].wait_recv()
        aside[i].start()

    jobs = {
        (1, 1): [functools.partial(share_own, 1)],
        (2, 1): [functools.partial(share_own, 2)],
        (3, 1): [functools.partial(share_own, 3)],
        (1, 3): [convolve, functools.partial(filter_rows, 0)],
        (1, 5): [functools.partial(filter_rows, half)],
        (1, 7): [statistics],
        (3, 4): [normalize],
        (4, 1): [functools.partial(share_onward, 0)],
        (5, 1): [functools.partial(share_onward, 1)],
        (6, 0): [functools.partial(share_aside, 0)],
        (7, 0): [functools.partial(share_aside, 1)],
        (8, 0): [functools.partial(share_aside, 2)],
    }
    for tile in range(tiles):
        jobs[4, 3 + tile] = jobs.get((4, 3 + tile), []) + [functools.partial(project, tile)]
        jobs[5, 3 + tile] = jobs.get((5, 3 + tile), []) + [functools.partial(reduce_pairs, tile)]
    last = max(dist + 1, 9)

    @pl.loop(1, last + 1)
    def _(step):
        plus_block = me - step
        minus_block = lax.rem(me + step, n)
        got_plus = (plus_block >= 0) & (step <= dist)
        got_minus = minus_gets(me, step)
        past_plus = plus_block + 1
        past_minus = lax.rem(me + step - 1, n)
        has_plus = (past_plus >= 0) & (step > 1) & (step <= dist + 1)
        has_minus = minus_gets(me, step - 1) & (step > 1) & (me > past_minus)
        plus_arrived = hop(plus_block, step - 1, True)
        plus_onward = hop(plus_block, step, True)
        minus_arrived = hop(minus_block, step - 1, False)
        minus_onward = hop(minus_block, step, False)

        for i in range(8):
            piece, rest = divmod(i * piece_count, 8)

            if rest == 0:

                @pl.when(got_plus)
                def _():
                    plus_arrived[piece].wait_recv()

                @pl.when(got_plus & plus_sends(step))
                def _():
                    plus_onward[piece].start()

                @pl.when(got_minus)
                def _():
                    minus_arrived[piece].wait_recv()

                @pl.when(got_minus & minus_sends(step))
                def _():
                    minus_onward[piece].start()

            if i == 2:

                @pl.when(has_plus)
                def _():
                    for chunk in range(chunks):
                        at, part_sum, lost = attend(past_plus, chunk, None)
                        seen = sum_r[at]
                        acc_r[at] = acc_r[at] + jnp.exp(-seen) * part_sum
                        sum_r[at] = seen + lost

            if i == 6:

                @pl.when(has_minus)
                def _():
                    for chunk in range(chunks):
                        at, part_sum, lost = attend(past_minus, chunk, None)
                        acc_l[at] = part_sum + jnp.exp(-lost) * acc_l[at]
                        sum_l[at] = sum_l[at] + lost

            for at_step, at_piece in jobs:
                if at_piece == i:

                    @pl.when(step == at_step)
                    def _():
                        for job in jobs[at_step, at_piece]:
                            job()

    finish()
    for q in range(2):
        for copy in onward_part(q):
            copy.wait_recv()
    aside[3].start()
    for tile in range(tiles):
        columns = slice(tile * span, (tile + 1) * span)
        total = conv_sum[:, columns]
        pltpu.make_async_remote_copy(
            src_ref=both.at[pl.ds(1, chips - 1), :, columns],
            dst_ref=recv.at[pl.ds(1, chips - 1), :, columns],
            send_sem=rs_ssem.at[tile],
            recv_sem=rs_rsem.at[tile],
            device_id={"tp": sibling},
            device_id_type=MESH,
        ).wait()
        for r in range(1, chips):
            total = total + recv[r, :, columns].astype(f32)
        conv_sum[:, columns] = total
    for copy in aside:
        copy.wait_recv()
    spread(12, 0, sibling, 0, 4 * width + 12 * fold).wait_send()
    pltpu.make_async_remote_copy(
        src_ref=head_send.at[pl.ds(1, tps - 1)],
        dst_ref=head_recv.at[pl.ds(1, tps - 1)],
        send_sem=side_sem.at[2],
        recv_sem=side_sem.at[3],
        device_id={"tp": sibling},
        device_id_type=MESH,
    ).wait()
    all_heads = jnp.concatenate([head_recv[i] for i in range(tps)], axis=1)
    for tile in range(tiles):
        columns = slice(tile * span, (tile + 1) * span)
        product = jnp.dot(all_heads, wa[:, columns], preferred_element_type=f32)
        out_ref[:, columns] = (product + conv_sum[:, columns]).astype(bf16)

    @pl.when(me < n - 1)
    def _():
        halo_copy.wait_send()

    @pl.loop(0, dist)
    def _(step):
        @pl.when(plus_sends(step))
        def _():
            whole(me - step, step, True).wait_send()

        @pl.when(minus_sends(step))
        def _():
            whole(lax.rem(me + step, n), step, False).wait_send()


def local(n, tps, stream, norm_gain, wq, wk, wv, wi, wg, offset, head_gain, taps, cgain, cshift, ao, fo):
    rows, features = stream.shape[1:]
    width = wq.shape[1]
    dist = n // 2
    dma = pltpu.SemaphoreType.DMA
    vmem = pl.BlockSpec(memory_space=pltpu.VMEM)
    anywhere = pl.BlockSpec(memory_space=pltpu.HBM)
    mixed, mass = pl.pallas_call(
        functools.partial(kernel, n, tps),
        out_shape=(
            jax.ShapeDtypeStruct((rows // tps, features), bf16),
            jax.ShapeDtypeStruct((2, rows), f32),
        ),
        in_specs=[anywhere] * 14,
        out_specs=(vmem, vmem),
        scratch_shapes=[
            pltpu.VMEM((rows, features), bf16),
            pltpu.VMEM((features,), bf16),
            pltpu.VMEM((width,), bf16),
            pltpu.VMEM(taps.shape, bf16),
            pltpu.VMEM((width,), bf16),
            pltpu.VMEM((width,), bf16),
            pltpu.VMEM((rows, features), bf16),
            pltpu.VMEM((features, 5 * width), bf16),
            pltpu.VMEM((tps * width, features), bf16),
            pltpu.VMEM((width, features), bf16),
            pltpu.VMEM((n, lead + 2 * rows, width), bf16),
            pltpu.VMEM((2, rows), bf16),
            pltpu.VMEM((2 * rows, width), bf16),
            pltpu.VMEM((rows, rows), bf16),
            pltpu.VMEM((2 * rows, width), f32),
            pltpu.VMEM((2 * rows, width), f32),
            pltpu.VMEM((2 * rows, width), f32),
            pltpu.VMEM((2 * rows, width), f32),
            pltpu.VMEM((rows, width), bf16),
            pltpu.VMEM((32, width), bf16),
            pltpu.VMEM((rows + 32, width), f32),
            pltpu.VMEM((rows, width), f32),
            pltpu.VMEM((8, rows), f32),
            pltpu.VMEM((tps, 8, rows), f32),
            pltpu.VMEM((rows, width), bf16),
            pltpu.VMEM((tps // 2, 2, rows // tps, features), bf16),
            pltpu.VMEM((tps // 2, rows // tps, features), bf16),
            pltpu.VMEM((tps // 2, rows // tps, features), bf16),
            pltpu.VMEM((tps // 2, rows // tps, features), bf16),
            pltpu.VMEM((rows // tps, features), f32),
            pltpu.VMEM((tps, rows // tps, width), bf16),
            pltpu.VMEM((tps, rows // tps, width), bf16),
            dma((14,)),
            dma((dist,)),
            dma((dist, piece_count)),
            dma((dist,)),
            dma((dist, piece_count)),
            dma((2,)),
            dma((2, 4)),
            dma((4,)),
            dma((4,)),
            dma((16,)),
            dma((5,)),
        ],
        compiler_params=pltpu.CompilerParams(
            collective_id=0, has_side_effects=True, vmem_limit_bytes=48000000
        ),
        name="layer",
    )(*[pltpu.with_memory_space_constraint(a, pltpu.HBM) for a in (stream[0], norm_gain, wq, wk, wv, wi, wg, offset[0].T, head_gain, taps, cgain, cshift, ao, fo)])
    return mixed[None], mass.T[None]


def solution(mesh):
    return jax.shard_map(
        functools.partial(local, mesh.shape["sp"], mesh.shape["tp"]),
        mesh=mesh,
        in_specs=(
            P("fs", "sp", None),
            P(),
            P(None, "tp"),
            P(None, "tp"),
            P(None, "tp"),
            P(None, "tp"),
            P(None, "tp"),
            P("fs", "sp", "tp"),
            P("tp"),
            P(None, "tp"),
            P("tp"),
            P("tp"),
            P("tp", None),
            P("tp", None),
        ),
        out_specs=(P("fs", ("sp", "tp"), None), P("fs", "sp", "tp")),
        check_vma=False,
    )
```

```python
import functools

import jax
import jax.numpy as jnp
from jax import lax
from jax.experimental import pallas as pl
from jax.experimental.pallas import tpu as pltpu
from jax.sharding import PartitionSpec as P

HEAD_DIM = 64

rms_eps = 1e-06
norm_eps = 1e-05
mass_floor = 0.01
piece_count = 4
lead = 16

MESH = pl.DeviceIdType.MESH
f32 = jnp.float32
bf16 = jnp.bfloat16


def dot_nt(a, b):
    return lax.dot_general(a, b, (((1,), (1,)), ((), ())), preferred_element_type=f32)


def kernel(
    n,
    tps,
    x_hbm,
    gain_hbm,
    wq_hbm,
    wk_hbm,
    wv_hbm,
    wi_hbm,
    wg_hbm,
    off_hbm,
    head_gain_hbm,
    taps_hbm,
    cgain_hbm,
    cshift_hbm,
    ao_hbm,
    fo_hbm,
    out_ref,
    mass_ref,
    x_v,
    gain_ref,
    head_gain_ref,
    taps_ref,
    cgain_ref,
    cshift_ref,
    normed,
    w_v,
    wa,
    fo_v,
    keep,
    off_v,
    qs,
    tri,
    acc_r,
    sum_r,
    acc_l,
    sum_l,
    gated,
    halo,
    ext,
    filt,
    stat_send,
    stat_recv,
    conv_v,
    part,
    pair,
    both,
    recv,
    conv_sum,
    head_send,
    head_recv,
    load_sem,
    plus_send,
    plus_recv,
    minus_send,
    minus_recv,
    halo_sem,
    pair_sem,
    rs_ssem,
    rs_rsem,
    gather_rsem,
    side_sem,
):
    rows = x_hbm.shape[0]
    width = wq_hbm.shape[1]
    reach = taps_ref.shape[0] - 1
    me = lax.axis_index("sp")
    tp = lax.axis_index("tp")
    right = lax.rem(me + 1, n)
    left = lax.rem(me + n - 1, n)
    dist = n // 2
    low = n - dist - 2

    barrier = pltpu.get_barrier_semaphore()
    for neighbour in (left, right):
        pl.semaphore_signal(barrier, inc=1, device_id={"sp": neighbour}, device_id_type=MESH)
    for r in range(1, tps):
        pl.semaphore_signal(
            barrier, inc=1, device_id={"tp": lax.rem(tp + r, tps)}, device_id_type=MESH
        )

    def rows_of(device):
        return pl.ds(pl.multiple_of(device * width, width), width)

    loads = [
        (x_hbm, x_v),
        (gain_hbm, gain_ref),
        (off_hbm, off_v),
        (wk_hbm, w_v.at[:, 0:width]),
        (wv_hbm, w_v.at[:, width : 2 * width]),
        (wq_hbm, w_v.at[:, 2 * width : 3 * width]),
        (wi_hbm, w_v.at[:, 3 * width : 4 * width]),
        (wg_hbm, w_v.at[:, 4 * width : 5 * width]),
        (ao_hbm, wa.at[rows_of(tp)]),
        (fo_hbm, fo_v),
        (taps_hbm, taps_ref),
        (head_gain_hbm, head_gain_ref),
        (cgain_hbm, cgain_ref),
        (cshift_hbm, cshift_ref),
    ]
    copies = [
        pltpu.make_async_copy(src, dst, load_sem.at[i]) for i, (src, dst) in enumerate(loads)
    ]
    for copy in copies[0:5]:
        copy.start()

    half = rows // 2

    block_rows = lead + 2 * rows
    bounds = [0] + [lead + i * 2 * rows // piece_count for i in range(1, piece_count + 1)]

    def send_piece(slot, step, plus, start, size, i):
        piece = keep.at[slot, pl.ds(start, size)]
        ssem, rsem = (plus_send, plus_recv) if plus else (minus_send, minus_recv)
        return pltpu.make_async_remote_copy(
            src_ref=piece,
            dst_ref=piece,
            send_sem=ssem.at[step],
            recv_sem=rsem.at[step, i],
            device_id={"sp": right if plus else left},
            device_id_type=MESH,
        )

    def hop(slot, step, plus):
        return [
            send_piece(slot, step, plus, bounds[i], bounds[i + 1] - bounds[i], i)
            for i in range(piece_count)
        ]

    def whole(slot, step, plus):
        return send_piece(slot, step, plus, 0, block_rows, 0)

    def plus_sends(step):
        return (me - step >= 0) & (me < n - 1) & (step < dist)

    def minus_gets(device, step):
        block = lax.rem(device + step, n)
        return (step < dist) & (block <= low) & ((device < block) | (device > block + dist))

    def minus_sends(step):
        block = lax.rem(me + step, n)
        fits = (step == 0) | minus_gets(me, step)
        return fits & (block <= low) & minus_gets(left, step + 1)

    row_id = lax.broadcasted_iota(jnp.int32, (rows, rows), 0)
    col_id = lax.broadcasted_iota(jnp.int32, (rows, rows), 1)
    tri[...] = (row_id > col_id).astype(f32).astype(bf16)

    copies[1].wait()
    gain = gain_ref[...].astype(f32).reshape(1, gain_ref.shape[0])
    copies[0].wait()
    for copy in copies[5:]:
        copy.start()

    @pl.loop(0, rows // 32)
    def _(i):
        at = pl.ds(pl.multiple_of(i * 32, 32), 32)
        xf = x_v[at].astype(f32)
        scale = lax.rsqrt(jnp.mean(xf * xf, axis=-1, keepdims=True) + rms_eps)
        normed[at] = (xf * scale * gain).astype(bf16)

    for i in (2, 3, 4):
        copies[i].wait()
    kv = jnp.dot(normed[...], w_v[:, 0 : 2 * width], preferred_element_type=f32)
    keep[me, lead : lead + rows] = kv[:, 0:width].astype(bf16)
    keep[me, lead + rows : block_rows] = kv[:, width : 2 * width].astype(bf16)
    offsets = off_v[...].astype(f32)
    lines = [offsets[h : h + 1, i : i + width] for h in range(2) for i in range(0, rows, width)]
    lines.append(jnp.zeros((lead - len(lines), width), f32))
    keep[me, 0:lead] = jnp.concatenate(lines, axis=0).astype(bf16)

    pl.semaphore_wait(barrier, tps + 1)

    @pl.when(plus_sends(0))
    def _():
        for copy in hop(me, 0, True):
            copy.start()

    @pl.when(minus_sends(0))
    def _():
        for copy in hop(me, 0, False):
            copy.start()

    chips = tps // 2
    chip, core = tp // 2, lax.rem(tp, 2)
    sibling = tp + 1 - 2 * core
    ahead = 2 * lax.rem(chip + 1, chips) + core
    behind = 2 * lax.rem(chip + chips - 1, chips) + core
    across = 2 * lax.rem(chip + 2, chips) + core
    fold = width // 4

    def spread(i, device, to, start=0, size=width):
        part_rows = wa.at[pl.ds(pl.multiple_of(device * width + start, fold), size)]
        return pltpu.make_async_remote_copy(
            src_ref=part_rows,
            dst_ref=part_rows,
            send_sem=side_sem.at[4],
            recv_sem=gather_rsem.at[i],
            device_id={"tp": to},
            device_id_type=MESH,
        )

    def own_part(q):
        return (
            spread(q, tp, ahead, q * fold, fold),
            spread(4 + q, tp, behind, lax.rem(q + 2, 4) * fold, fold),
        )

    def onward_part(q):
        return (
            spread(8 + q, behind, ahead, q * fold, fold),
            spread(10 + q, ahead, behind, (q + 2) * fold, fold),
        )

    aside = [spread(12 + i, device, sibling) for i, device in enumerate((tp, behind, ahead, across))]
    copies[8].wait()
    for copy in own_part(0):
        copy.start()

    for i in (5, 6, 7):
        copies[i].wait()
    qig = jnp.dot(normed[...], w_v[:, 2 * width : 5 * width], preferred_element_type=f32)
    gate = qig[:, 2 * width : 3 * width].astype(bf16).astype(f32)
    conv_in = qig[:, width : 2 * width].astype(bf16).astype(f32)
    gated_rows = (conv_in * (1.0 / (1.0 + jnp.exp(-gate)))).astype(bf16)
    gated[...] = gated_rows
    tail = 32
    halo_copy = pltpu.make_async_remote_copy(
        src_ref=gated.at[pl.ds(rows - tail, tail)],
        dst_ref=halo,
        send_sem=halo_sem.at[0],
        recv_sem=halo_sem.at[1],
        device_id={"sp": right},
        device_id_type=MESH,
    )

    @pl.when(me < n - 1)
    def _():
        halo_copy.start()

    lane = lax.broadcasted_iota(jnp.int32, (rows, width), 1)
    first = lane < HEAD_DIM
    query = qig[:, 0:width].astype(bf16).astype(f32) * HEAD_DIM ** (-0.5)
    qs[0:rows] = jnp.where(first, query, 0.0).astype(bf16)
    qs[rows : 2 * rows] = jnp.where(first, 0.0, query).astype(bf16)

    def attend(slot, chunk, strict):
        at = pl.ds(0, 2 * rows)
        lines = keep[slot, 0:lead].astype(f32)
        per_head = rows // width
        offset = jnp.concatenate(
            [
                jnp.broadcast_to(
                    jnp.concatenate(
                        [lines[head * per_head + i : head * per_head + i + 1] for i in range(per_head)],
                        axis=1,
                    ),
                    (rows, rows),
                )
                for head in range(2)
            ],
            axis=0,
        )
        scores = dot_nt(qs[at], keep[slot, lead : lead + rows]) + offset
        soft = jnp.maximum(jnp.log(1.0 + jnp.exp(jnp.minimum(scores, 80.0))), scores)
        gain_log = scores - soft
        if strict is not None:
            soft = jnp.where(strict, soft, 0.0)
        beyond = jnp.dot(soft.astype(bf16), tri[...], preferred_element_type=f32)
        weights = jnp.exp(gain_log - beyond)
        if strict is not None:
            weights = jnp.where(strict, weights, 0.0)
        part_sum = jnp.dot(weights.astype(bf16), keep[slot, lead + rows : block_rows], preferred_element_type=f32)
        lost = jnp.broadcast_to(beyond[:, 0:1] + soft[:, 0:1], (2 * rows, width))
        return at, part_sum, lost

    chunks = 1
    for chunk in range(chunks):
        at, part_sum, lost = attend(me, chunk, jnp.concatenate([col_id < row_id] * 2, axis=0))
        acc_r[at] = part_sum
        sum_r[at] = lost
    for i in (10, 11, 12, 13):
        copies[i].wait()
    acc_l[...] = jnp.zeros_like(acc_l)
    sum_l[...] = jnp.zeros_like(sum_l)

    stat_copies = [
        pltpu.make_async_remote_copy(
            src_ref=stat_send,
            dst_ref=stat_recv.at[r],
            send_sem=side_sem.at[0],
            recv_sem=side_sem.at[1],
            device_id={"tp": lax.rem(tp + r, tps)},
            device_id_type=MESH,
        )
        for r in range(1, tps)
    ]

    def convolve():
        @pl.when(me > 0)
        def _():
            halo_copy.wait_recv()
            ext[0:tail] = halo[...].astype(f32)

        @pl.when(me == 0)
        def _():
            ext[0:tail] = jnp.zeros((tail, width), f32)

        ext[tail : tail + rows] = gated[...].astype(f32)

    def filter_rows(base):
        taps = taps_ref[...].astype(f32)
        total = jnp.zeros((half, width), f32)
        for k in range(reach + 1):
            total = total + ext[base + tail - reach + k : base + tail - reach + k + half] * taps[k : k + 1]
        filt[base : base + half] = total

    def statistics():
        filtered = filt[...]
        sums = jnp.sum(filtered, axis=-1, keepdims=True)
        squares = jnp.sum(filtered * filtered, axis=-1, keepdims=True)
        packed = jnp.where(lane == 0, sums, squares)
        stat_send[...] = packed.T[0:8]
        for copy in stat_copies:
            copy.start()

    def normalize():
        total = stat_send[...]
        pltpu.make_async_remote_copy(
            src_ref=stat_recv.at[pl.ds(1, tps - 1)],
            dst_ref=stat_recv.at[pl.ds(1, tps - 1)],
            send_sem=side_sem.at[0],
            recv_sem=side_sem.at[1],
            device_id={"tp": sibling},
            device_id_type=MESH,
        ).wait()
        for r in range(1, tps):
            total = total + stat_recv[r]
        mean = total / (width * tps)
        center = mean[0:1]
        spread = jnp.maximum(mean[1:2] - center * center, 0.0)
        scale = lax.rsqrt(spread + norm_eps)
        line = lax.broadcasted_iota(jnp.int32, (width, rows), 0)
        columns = jnp.where(line == 0, center, scale).T
        hidden = (filt[...] - columns[:, 0:1]) * columns[:, 1:2]
        hidden = hidden * cgain_ref[...].astype(f32).reshape(1, width)
        hidden = hidden + cshift_ref[...].astype(f32).reshape(1, width)
        conv_v[...] = (hidden * (1.0 / (1.0 + jnp.exp(-hidden)))).astype(bf16)
        copies[9].wait()

    features = wa.shape[1]
    share = rows // tps
    tiles = 4
    span = features // tiles

    def swap(tile):
        columns = pl.ds(tile * span, span)
        return pltpu.make_async_remote_copy(
            src_ref=part.at[:, 1 - core, :, columns],
            dst_ref=pair.at[:, :, columns],
            send_sem=pair_sem.at[0, tile],
            recv_sem=pair_sem.at[1, tile],
            device_id={"tp": sibling},
            device_id_type=MESH,
        )

    def exchange(tile, r):
        columns = pl.ds(tile * span, span)
        return pltpu.make_async_remote_copy(
            src_ref=both.at[r, :, columns],
            dst_ref=recv.at[r, :, columns],
            send_sem=rs_ssem.at[tile],
            recv_sem=rs_rsem.at[tile],
            device_id={"tp": 2 * lax.rem(chip + r, chips) + core},
            device_id_type=MESH,
        )

    def finish():
        attended = acc_r[...] + jnp.exp(-sum_r[...]) * acc_l[...]
        lost = sum_r[...] + sum_l[...]
        mass = jnp.log(jnp.maximum(1.0 - jnp.exp(-jnp.where(first, lost[0:rows], lost[rows : 2 * rows])), mass_floor)).T
        mass_ref[0:1] = mass[0:1]
        mass_ref[1:2] = mass[HEAD_DIM : HEAD_DIM + 1]
        attended = jnp.where(first, attended[0:rows], attended[rows : 2 * rows])
        power = attended * attended
        low_mean = jnp.sum(jnp.where(first, power, 0.0), axis=-1, keepdims=True) / HEAD_DIM
        high_mean = jnp.sum(jnp.where(first, 0.0, power), axis=-1, keepdims=True) / HEAD_DIM
        scale = jnp.where(first, lax.rsqrt(low_mean + rms_eps), lax.rsqrt(high_mean + rms_eps))
        heads = attended * scale * head_gain_ref[...].astype(f32).reshape(1, width)
        head_send[...] = heads.astype(bf16).reshape(tps, share, width)
        for r in range(1, tps):
            pass_heads(r).start()
        head_recv[tp] = head_send[tp]

    def pass_heads(r):
        peer = lax.rem(tp + r, tps)
        return pltpu.make_async_remote_copy(
            src_ref=head_send.at[peer],
            dst_ref=head_recv.at[tp],
            send_sem=side_sem.at[2],
            recv_sem=side_sem.at[3],
            device_id={"tp": peer},
            device_id_type=MESH,
        )

    def project(tile):
        columns = slice(tile * span, (tile + 1) * span)
        product = jnp.dot(conv_v[...], fo_v[:, columns], preferred_element_type=f32).astype(bf16)
        part[:, :, :, columns] = product.reshape(chips, 2, share, span)
        swap(tile).start()

    def reduce_pairs(tile):
        columns = slice(tile * span, (tile + 1) * span)
        swap(tile).wait()
        for r in range(chips):
            to = lax.rem(chip + r, chips)
            total = part[to, core, :, columns].astype(f32) + pair[to, :, columns].astype(f32)
            if r == 0:
                conv_sum[:, columns] = total
            else:
                both[r, :, columns] = total.astype(bf16)
                exchange(tile, r).start()

    def share_own(q):
        for copy in own_part(q):
            copy.start()

    def share_onward(q):
        for copy, ahead_copy in zip(own_part(q), onward_part(q)):
            copy.wait_recv()
            ahead_copy.start()

    def share_aside(i):
        if i > 0:
            for q in range(2, 4):
                own_part(q)[i - 1].wait_recv()
        aside[i].start()

    jobs = {
        (1, 1): [functools.partial(share_own, 1)],
        (2, 1): [functools.partial(share_own, 2)],
        (3, 1): [functools.partial(share_own, 3)],
        (1, 3): [convolve, functools.partial(filter_rows, 0)],
        (1, 5): [functools.partial(filter_rows, half)],
        (1, 7): [statistics],
        (3, 4): [normalize],
        (4, 1): [functools.partial(share_onward, 0)],
        (5, 1): [functools.partial(share_onward, 1)],
        (6, 0): [functools.partial(share_aside, 0)],
        (7, 0): [functools.partial(share_aside, 1)],
        (8, 0): [functools.partial(share_aside, 2)],
    }
    for tile in range(tiles):
        jobs[4, 3 + tile] = jobs.get((4, 3 + tile), []) + [functools.partial(project, tile)]
        jobs[5, 3 + tile] = jobs.get((5, 3 + tile), []) + [functools.partial(reduce_pairs, tile)]
    last = max(dist + 1, 9)

    @pl.loop(1, last + 1)
    def _(step):
        plus_block = me - step
        minus_block = lax.rem(me + step, n)
        got_plus = (plus_block >= 0) & (step <= dist)
        got_minus = minus_gets(me, step)
        past_plus = plus_block + 1
        past_minus = lax.rem(me + step - 1, n)
        has_plus = (past_plus >= 0) & (step > 1) & (step <= dist + 1)
        has_minus = minus_gets(me, step - 1) & (step > 1) & (me > past_minus)
        plus_arrived = hop(plus_block, step - 1, True)
        plus_onward = hop(plus_block, step, True)
        minus_arrived = hop(minus_block, step - 1, False)
        minus_onward = hop(minus_block, step, False)

        for i in range(8):
            piece, rest = divmod(i * piece_count, 8)

            if rest == 0:

                @pl.when(got_plus)
                def _():
                    plus_arrived[piece].wait_recv()

                @pl.when(got_plus & plus_sends(step))
                def _():
                    plus_onward[piece].start()

                @pl.when(got_minus)
                def _():
                    minus_arrived[piece].wait_recv()

                @pl.when(got_minus & minus_sends(step))
                def _():
                    minus_onward[piece].start()

            if i == 2:

                @pl.when(has_plus)
                def _():
                    for chunk in range(chunks):
                        at, part_sum, lost = attend(past_plus, chunk, None)
                        seen = sum_r[at]
                        acc_r[at] = acc_r[at] + jnp.exp(-seen) * part_sum
                        sum_r[at] = seen + lost

            if i == 6:

                @pl.when(has_minus)
                def _():
                    for chunk in range(chunks):
                        at, part_sum, lost = attend(past_minus, chunk, None)
                        acc_l[at] = part_sum + jnp.exp(-lost) * acc_l[at]
                        sum_l[at] = sum_l[at] + lost

            for at_step, at_piece in jobs:
                if at_piece == i:

                    @pl.when(step == at_step)
                    def _():
                        for job in jobs[at_step, at_piece]:
                            job()

    finish()
    for q in range(2):
        for copy in onward_part(q):
            copy.wait_recv()
    aside[3].start()
    for tile in range(tiles):
        columns = slice(tile * span, (tile + 1) * span)
        total = conv_sum[:, columns]
        pltpu.make_async_remote_copy(
            src_ref=both.at[pl.ds(1, chips - 1), :, columns],
            dst_ref=recv.at[pl.ds(1, chips - 1), :, columns],
            send_sem=rs_ssem.at[tile],
            recv_sem=rs_rsem.at[tile],
            device_id={"tp": sibling},
            device_id_type=MESH,
        ).wait()
        for r in range(1, chips):
            total = total + recv[r, :, columns].astype(f32)
        conv_sum[:, columns] = total
    for copy in aside:
        copy.wait_recv()
    spread(12, 0, sibling, 0, 4 * width + 12 * fold).wait_send()
    pltpu.make_async_remote_copy(
        src_ref=head_send.at[pl.ds(1, tps - 1)],
        dst_ref=head_recv.at[pl.ds(1, tps - 1)],
        send_sem=side_sem.at[2],
        recv_sem=side_sem.at[3],
        device_id={"tp": sibling},
        device_id_type=MESH,
    ).wait()
    all_heads = jnp.concatenate([head_recv[i] for i in range(tps)], axis=1)
    for tile in range(tiles):
        columns = slice(tile * span, (tile + 1) * span)
        product = jnp.dot(all_heads, wa[:, columns], preferred_element_type=f32)
        out_ref[:, columns] = (product + conv_sum[:, columns]).astype(bf16)

    @pl.when(me < n - 1)
    def _():
        halo_copy.wait_send()

    @pl.loop(0, dist)
    def _(step):
        @pl.when(plus_sends(step))
        def _():
            whole(me - step, step, True).wait_send()

        @pl.when(minus_sends(step))
        def _():
            whole(lax.rem(me + step, n), step, False).wait_send()


def local(n, tps, stream, norm_gain, wq, wk, wv, wi, wg, offset, head_gain, taps, cgain, cshift, ao, fo):
    rows, features = stream.shape[1:]
    width = wq.shape[1]
    dist = n // 2
    dma = pltpu.SemaphoreType.DMA
    vmem = pl.BlockSpec(memory_space=pltpu.VMEM)
    anywhere = pl.BlockSpec(memory_space=pltpu.HBM)
    mixed, mass = pl.pallas_call(
        functools.partial(kernel, n, tps),
        out_shape=(
            jax.ShapeDtypeStruct((rows // tps, features), bf16),
            jax.ShapeDtypeStruct((2, rows), f32),
        ),
        in_specs=[anywhere] * 14,
        out_specs=(vmem, vmem),
        scratch_shapes=[
            pltpu.VMEM((rows, features), bf16),
            pltpu.VMEM((features,), bf16),
            pltpu.VMEM((width,), bf16),
            pltpu.VMEM(taps.shape, bf16),
            pltpu.VMEM((width,), bf16),
            pltpu.VMEM((width,), bf16),
            pltpu.VMEM((rows, features), bf16),
            pltpu.VMEM((features, 5 * width), bf16),
            pltpu.VMEM((tps * width, features), bf16),
            pltpu.VMEM((width, features), bf16),
            pltpu.VMEM((n, lead + 2 * rows, width), bf16),
            pltpu.VMEM((2, rows), bf16),
            pltpu.VMEM((2 * rows, width), bf16),
            pltpu.VMEM((rows, rows), bf16),
            pltpu.VMEM((2 * rows, width), f32),
            pltpu.VMEM((2 * rows, width), f32),
            pltpu.VMEM((2 * rows, width), f32),
            pltpu.VMEM((2 * rows, width), f32),
            pltpu.VMEM((rows, width), bf16),
            pltpu.VMEM((32, width), bf16),
            pltpu.VMEM((rows + 32, width), f32),
            pltpu.VMEM((rows, width), f32),
            pltpu.VMEM((8, rows), f32),
            pltpu.VMEM((tps, 8, rows), f32),
            pltpu.VMEM((rows, width), bf16),
            pltpu.VMEM((tps // 2, 2, rows // tps, features), bf16),
            pltpu.VMEM((tps // 2, rows // tps, features), bf16),
            pltpu.VMEM((tps // 2, rows // tps, features), bf16),
            pltpu.VMEM((tps // 2, rows // tps, features), bf16),
            pltpu.VMEM((rows // tps, features), f32),
            pltpu.VMEM((tps, rows // tps, width), bf16),
            pltpu.VMEM((tps, rows // tps, width), bf16),
            dma((14,)),
            dma((dist,)),
            dma((dist, piece_count)),
            dma((max(dist - 1, 1),)),
            dma((max(dist - 1, 1), piece_count)),
            dma((2,)),
            dma((2, 4)),
            dma((4,)),
            dma((4,)),
            dma((16,)),
            dma((5,)),
        ],
        compiler_params=pltpu.CompilerParams(
            collective_id=0, has_side_effects=True, vmem_limit_bytes=48000000
        ),
        name="layer",
    )(*[pltpu.with_memory_space_constraint(a, pltpu.HBM) for a in (stream[0], norm_gain, wq, wk, wv, wi, wg, offset[0].T, head_gain, taps, cgain, cshift, ao, fo)])
    return mixed[None], mass.T[None]


def solution(mesh):
    return jax.shard_map(
        functools.partial(local, mesh.shape["sp"], mesh.shape["tp"]),
        mesh=mesh,
        in_specs=(
            P("fs", "sp", None),
            P(),
            P(None, "tp"),
            P(None, "tp"),
            P(None, "tp"),
            P(None, "tp"),
            P(None, "tp"),
            P("fs", "sp", "tp"),
            P("tp"),
            P(None, "tp"),
            P("tp"),
            P("tp"),
            P("tp", None),
            P("tp", None),
        ),
        out_specs=(P("fs", ("sp", "tp"), None), P("fs", "sp", "tp")),
        check_vma=False,
    )
```
